512 devices in a mesh: tp: 32 (over z, core), dp: 16 (over y, x).
Axes of the slice: x: 4, y: 4, z: 16, core: 2. Of those that a mesh axis runs over, the one named last changes fastest.
Arguments:
- incoming_embeddings: bfloat16 [96, 4096], P('tp', 'dp'), may hold values from -12 to 12
- rescale_factors: bfloat16 [2, 4096], P(None, 'dp'), may hold values from 0.099609375 to 1.8984375
- probe_lift: bfloat16 [2, 4096, 4096], P(None, 'dp', 'tp'), may hold values from -0.09375 to 0.09375
- address_lift: bfloat16 [2, 4096, 4096], P(None, 'dp', 'tp'), may hold values from -0.09375 to 0.09375
- forget_lift: bfloat16 [2, 4096, 4096], P(None, 'dp', 'tp'), may hold values from -0.09375 to 0.09375
- forget_shift: float32 [2, 4096], P(None, 'tp'), may hold values from -6 to 3
- surplus_fade: float32 [2, 96, 4096], P(None, 'dp', 'tp'), may hold values from -0.7 to 0
- content_lift: bfloat16 [2, 4096, 8192], P(None, 'dp', 'tp'), may hold values from -0.09375 to 0.09375
- filter_lift: bfloat16 [2, 4096, 8192], P(None, 'dp', 'tp'), may hold values from -0.09375 to 0.09375
- readback_lift: bfloat16 [2, 8192, 4096], P(None, 'tp', 'dp'), may hold values from -0.0625 to 0.0625
- memory_tensor: float32 [2, 96, 128, 8192], P(None, 'dp', None, 'tp'), may hold values from -6 to 6
Outputs:
- mixed: bfloat16 [96, 4096], P('tp', 'dp')
- new_state: float32 [2, 96, 128, 8192], P(None, 'dp', None, 'tp')
The draws below stay inside these ranges and needn't reach their ends.
All inputs are finite; a program needn't handle non-finite values.
Results may differ from the reference program's by a relative error of at most 0.0085.
Values may be sent and summed in bfloat16 or wider, within the bound.
No kernel may reach another device: no remote copies, remote signals or barrier semaphores. Data moves between devices by JAX's collectives and lax.ppermute only.
A program may use at most 64 MiB of HBM per device.

```python
import math
import jax
import jax.numpy as jnp
from jax import lax

D = 4096
HEADS = 32
DK = 128
DV = 256
BLOCKS = 2
KW = 4096
VW = 8192
SEQS = 96


def draw_incoming_embeddings(key, part):
    first_key = jax.random.fold_in(jax.random.fold_in(key, 11), 0)
    col_scale = jnp.exp(jnp.linspace(math.log(0.5), math.log(2.5), D)).astype(jnp.float32)
    base_draw = jax.random.normal(first_key, (SEQS, D), jnp.float32)
    return jnp.clip(base_draw * col_scale, -12.0, 12.0).astype(jnp.bfloat16)


def draw_surplus_fade(key, part):
    first_key, second_key = jax.random.split(jax.random.fold_in(key, 23))
    hit_mask = jax.random.randint(first_key, (BLOCKS, SEQS, KW), 0, 8) == 0
    drop_size = jax.random.uniform(second_key, (BLOCKS, SEQS, KW), jnp.float32, -0.7, -0.22)
    return jnp.where(hit_mask, drop_size, 0.0).astype(jnp.float32)


def block_levels(own_key, dims, cuts, least, top_value):
    factor_of = 1.0
    for position, parts in cuts:
        draws = jax.random.uniform(jax.random.fold_in(jax.random.fold_in(own_key, 6), position), (parts,), jnp.float32, least / len(cuts), top_value / len(cuts))
        factor_of = factor_of * jnp.repeat(jnp.exp(draws), dims[position] // parts).reshape((-1,) + (1,) * (len(dims) - 1 - position))
    return factor_of


def normal_values(key, dims, width, bound, cuts=(), kind=jnp.bfloat16):
    gain = block_levels(key, dims, cuts, -0.22, 0.18) if cuts else 1.0
    array = jax.random.normal(key, dims, jnp.float32) * width * gain
    return jnp.minimum(jnp.maximum(array, -bound), bound).astype(kind)


def setup_inputs(seed: int = 0) -> dict:
    streams_of = jax.random.split(jax.random.key(seed), 12)
    return {
        "incoming_embeddings": draw_incoming_embeddings(jax.random.fold_in(streams_of[11], 71), 0),
        "rescale_factors": jnp.clip(1.0 + 0.18 * jax.random.normal(streams_of[1], (BLOCKS, D), jnp.float32), 0.099609375, 1.8984375).astype(jnp.bfloat16),
        "probe_lift": normal_values(streams_of[2], (BLOCKS, D, KW), D ** -0.5, 0.09375, ((1, 16), (2, 32))),
        "address_lift": normal_values(streams_of[3], (BLOCKS, D, KW), D ** -0.5, 0.09375, ((1, 16), (2, 32))),
        "forget_lift": normal_values(streams_of[4], (BLOCKS, D, KW), D ** -0.5, 0.09375, ((1, 16), (2, 32))),
        "forget_shift": jnp.clip(-6.0 + 9.0 * jax.random.uniform(streams_of[5], (BLOCKS, KW), jnp.float32) ** block_levels(streams_of[5], (BLOCKS, KW), ((1, 32),), -0.2, 0.2), -6.0, 3.0),
        "surplus_fade": draw_surplus_fade(jax.random.fold_in(streams_of[11], 71), 0),
        "content_lift": normal_values(streams_of[7], (BLOCKS, D, VW), D ** -0.5, 0.09375, ((1, 16), (2, 32))),
        "filter_lift": normal_values(streams_of[8], (BLOCKS, D, VW), D ** -0.5, 0.09375, ((1, 16), (2, 32))),
        "readback_lift": normal_values(streams_of[9], (BLOCKS, VW, D), VW ** -0.5, 0.0625, ((1, 32), (2, 16))),
        "memory_tensor": normal_values(streams_of[10], (BLOCKS, SEQS, DK, VW), 1.0, 6.0, ((1, 16), (3, 32)), jnp.float32),
    }


def reference(incoming_embeddings, rescale_factors, probe_lift, address_lift, forget_lift, forget_shift, surplus_fade, content_lift, filter_lift, readback_lift, memory_tensor):
    stream = incoming_embeddings
    collected = []
    seq_count = incoming_embeddings.shape[0]
    for layer_ordinal in range(BLOCKS):
        resid = stream.astype(jnp.float32)
        inv_rms = lax.rsqrt(lax.optimization_barrier(jnp.sum(resid * resid, axis=1, keepdims=True)) / D + 1e-06)
        hidden = (resid * rescale_factors[layer_ordinal].astype(jnp.float32)).astype(jnp.bfloat16)

        def linear_map_step(matrix):
            return inv_rms * jnp.dot(hidden, matrix[layer_ordinal], preferred_element_type=jnp.float32)
        queries = linear_map_step(probe_lift) * DK ** (-0.5)
        key_vals = linear_map_step(address_lift)
        values = linear_map_step(content_lift)
        gate_vals = linear_map_step(filter_lift)
        forget_rate_ln = jax.nn.log_sigmoid(linear_map_step(forget_lift) + forget_shift[layer_ordinal]) / 16.0 + surplus_fade[layer_ordinal]
        old_state = memory_tensor[layer_ordinal].reshape(seq_count, DK, HEADS, DV)
        decays = jnp.transpose(jnp.exp(forget_rate_ln).reshape(seq_count, HEADS, DK), (0, 2, 1))
        key_heads = key_vals.reshape(seq_count, HEADS, DK)
        value_heads = values.reshape(seq_count, HEADS, DV)
        fresh = old_state * decays[..., None] + jnp.einsum('shk,she->skhe', key_heads, value_heads, precision=lax.Precision.HIGHEST)
        readout = jnp.einsum('shk,skhe->she', queries.reshape(seq_count, HEADS, DK), fresh, precision=lax.Precision.HIGHEST).reshape(seq_count, VW)
        gated = (readout * jax.nn.silu(gate_vals)).astype(jnp.bfloat16)
        branch = jnp.dot(gated, readback_lift[layer_ordinal], preferred_element_type=jnp.float32)
        stream = (resid + branch).astype(jnp.bfloat16)
        collected.append(fresh.reshape(seq_count, DK, VW))
    return (stream, jnp.stack(collected))
```

```python
import jax
import jax.numpy as jnp
from jax import lax
from jax.sharding import Mesh, PartitionSpec as P

D = 4096
DK = 128
BLOCKS = 2
PAD = 8
BF = jnp.bfloat16
F32 = jnp.float32
DP = ("y", "x")
TP = ("z", "c")


def exchange(parts, axis):
    return lax.all_to_all(parts, axis, 0, 0, tiled=True)


def everyone(rows, axis):
    return exchange(jnp.broadcast_to(rows[None], (lax.axis_size(axis), *rows.shape)), axis)


def pad_rows(rows):
    return jnp.pad(rows, ((0, PAD - rows.shape[0]), (0, 0)))


def shards(
    incoming_embeddings,
    rescale_factors,
    probe_lift,
    address_lift,
    forget_lift,
    forget_shift,
    surplus_fade,
    content_lift,
    filter_lift,
    readback_lift,
    memory_tensor,
):
    kc = probe_lift.shape[2]
    vc = content_lift.shape[2]
    cols = 3 * kc + 2 * vc
    seqs = memory_tensor.shape[1]
    groups = lax.axis_size(DP)
    core = lax.axis_index("c")
    stream = pad_rows(lax.all_gather(incoming_embeddings, "c", axis=0, tiled=True))
    fresh_all = []
    for b in range(BLOCKS):
        weights = jnp.concatenate(
            [
                probe_lift[b],
                address_lift[b],
                forget_lift[b],
                content_lift[b],
                filter_lift[b],
                jnp.zeros((probe_lift.shape[1], 128), BF),
            ],
            axis=1,
        )
        rows = everyone(stream, "z").astype(F32).reshape(groups * PAD, -1)
        hidden = (rows * rescale_factors[b].astype(F32)).astype(BF)
        squares = jnp.sum(rows * rows, axis=1, keepdims=True)
        partial = jnp.dot(hidden, weights, preferred_element_type=F32)
        column = lax.broadcasted_iota(jnp.int32, partial.shape, 1)
        partial = jnp.where(column == cols, squares, partial).astype(BF)
        parts = exchange(partial.reshape(groups, PAD, -1), DP)
        total = jnp.sum(parts.astype(F32), axis=0)[:seqs]
        inv_rms = lax.rsqrt(total[:, cols : cols + 1] / D + 1e-06)
        projected = total[:, :cols] * inv_rms
        queries = projected[:, :kc] * DK ** (-0.5)
        keys = projected[:, kc : 2 * kc]
        decay_pre = projected[:, 2 * kc : 3 * kc] + forget_shift[b]
        values = projected[:, 3 * kc : 3 * kc + vc]
        gates = projected[:, 3 * kc + vc :]
        decay = jnp.exp(jax.nn.log_sigmoid(decay_pre) / 16.0 + surplus_fade[b])
        fresh = memory_tensor[b] * decay[:, :, None] + keys[:, :, None] * values[:, None, :]
        readout = jnp.sum(queries[:, :, None] * fresh, axis=1)
        gated = (readout * jax.nn.silu(gates)).astype(BF)
        fresh_all.append(fresh)
        gathered = everyone(pad_rows(gated), DP).reshape(groups * PAD, vc)
        branch = jnp.dot(gathered, readback_lift[b], preferred_element_type=F32)
        heads = exchange(branch.astype(BF).reshape(groups, PAD, -1), "z")
        own = jnp.sum(heads.astype(F32), axis=0)
        both = lax.all_gather(own, "c", axis=0)
        stream = (stream.astype(F32) + (both[0] + both[1])).astype(BF)
    third = incoming_embeddings.shape[0]
    mixed = jnp.where(core == 0, stream[:third], stream[third : 2 * third])
    return mixed, jnp.stack(fresh_all)


def solution(mesh):
    sizes = dict(mesh.shape)
    z = sizes["tp"] // 2
    y = x = 4
    fine = Mesh(mesh.devices.reshape(z, 2, y, x), ("z", "c", "y", "x"))
    in_specs = (
        P(TP, DP),
        P(None, DP),
        P(None, DP, TP),
        P(None, DP, TP),
        P(None, DP, TP),
        P(None, TP),
        P(None, DP, TP),
        P(None, DP, TP),
        P(None, DP, TP),
        P(None, TP, DP),
        P(None, DP, None, TP),
    )
    out_specs = (P(TP, DP), P(None, DP, None, TP))
    return jax.shard_map(shards, mesh=fine, in_specs=in_specs, out_specs=out_specs, check_vma=False)
```

```python
import jax
import jax.numpy as jnp
from jax import lax
from jax.sharding import Mesh, PartitionSpec as P

D = 4096
DK = 128
BLOCKS = 2
PAD = 8
BF = jnp.bfloat16
F32 = jnp.float32
DP = ("y", "x")
TP = ("z", "c")


def exchange(parts, axis):
    return lax.all_to_all(parts, axis, 0, 0, tiled=True)


def everyone(rows, axis):
    return exchange(jnp.broadcast_to(rows[None], (lax.axis_size(axis), *rows.shape)), axis)


def pad_rows(rows):
    return jnp.pad(rows, ((0, PAD - rows.shape[0]), (0, 0)))


def shards(
    incoming_embeddings,
    rescale_factors,
    probe_lift,
    address_lift,
    forget_lift,
    forget_shift,
    surplus_fade,
    content_lift,
    filter_lift,
    readback_lift,
    memory_tensor,
):
    kc = probe_lift.shape[2]
    vc = content_lift.shape[2]
    cols = 3 * kc + 2 * vc
    seqs = memory_tensor.shape[1]
    groups = lax.axis_size(DP)
    core = lax.axis_index("c")
    stream = pad_rows(lax.all_gather(incoming_embeddings, "c", axis=0, tiled=True))
    fresh_all = []
    ready = [
        (
            jnp.concatenate(
                [
                    probe_lift[b],
                    address_lift[b],
                    forget_lift[b],
                    content_lift[b],
                    filter_lift[b],
                    jnp.zeros((probe_lift.shape[1], 128), BF),
                ],
                axis=1,
            ),
            rescale_factors[b].astype(F32),
            forget_shift[b],
            surplus_fade[b],
            readback_lift[b],
            memory_tensor[b],
        )
        for b in range(BLOCKS)
    ]
    for b in range(BLOCKS):
        rows = everyone(stream, "z")
        if b == 0:
            rows, ready, core = lax.optimization_barrier((rows, ready, core))
        weights, gain, shift, fade, back, memory = ready[b]
        rows = rows.astype(F32).reshape(groups * PAD, -1)
        hidden = (rows * gain).astype(BF)
        squares = jnp.sum(rows * rows, axis=1, keepdims=True)
        partial = jnp.dot(hidden, weights, preferred_element_type=F32)
        column = lax.broadcasted_iota(jnp.int32, partial.shape, 1)
        partial = jnp.where(column == cols, squares, partial).astype(BF)
        parts = exchange(partial.reshape(groups, PAD, -1), DP)
        total = jnp.sum(parts.astype(F32), axis=0)[:seqs]
        inv_rms = lax.rsqrt(total[:, cols : cols + 1] / D + 1e-06)
        projected = total[:, :cols] * inv_rms
        queries = projected[:, :kc] * DK ** (-0.5)
        keys = projected[:, kc : 2 * kc]
        decay_pre = projected[:, 2 * kc : 3 * kc] + shift
        values = projected[:, 3 * kc : 3 * kc + vc]
        gates = projected[:, 3 * kc + vc :]
        decay = jnp.exp(jax.nn.log_sigmoid(decay_pre) / 16.0 + fade)
        fresh = memory * decay[:, :, None] + keys[:, :, None] * values[:, None, :]
        readout = jnp.sum(queries[:, :, None] * fresh, axis=1)
        gated = (readout * jax.nn.silu(gates)).astype(BF)
        fresh_all.append(fresh)
        gathered = everyone(pad_rows(gated), DP).reshape(groups * PAD, vc)
        branch = jnp.dot(gathered, back, preferred_element_type=F32)
        heads = exchange(branch.astype(BF).reshape(groups, PAD, -1), "z")
        own = jnp.sum(heads.astype(F32), axis=0)
        both = lax.all_gather(own, "c", axis=0)
        stream = (stream.astype(F32) + (both[0] + both[1])).astype(BF)
    third = incoming_embeddings.shape[0]
    mixed = jnp.where(core == 0, stream[:third], stream[third : 2 * third])
    return mixed, jnp.stack(fresh_all)


def solution(mesh):
    sizes = dict(mesh.shape)
    z = sizes["tp"] // 2
    y = x = 4
    fine = Mesh(mesh.devices.reshape(z, 2, y, x), ("z", "c", "y", "x"))
    in_specs = (
        P(TP, DP),
        P(None, DP),
        P(None, DP, TP),
        P(None, DP, TP),
        P(None, DP, TP),
        P(None, TP),
        P(None, DP, TP),
        P(None, DP, TP),
        P(None, DP, TP),
        P(None, TP, DP),
        P(None, DP, None, TP),
    )
    out_specs = (P(TP, DP), P(None, DP, None, TP))
    return jax.shard_map(shards, mesh=fine, in_specs=in_specs, out_specs=out_specs, check_vma=False)
```

```python
import functools

import jax
import jax.numpy as jnp
from jax import lax
from jax.experimental import pallas as pl
from jax.experimental.pallas import tpu as pltpu
from jax.sharding import Mesh, PartitionSpec as P

D = 4096
DK = 128
BLOCKS = 2
PAD = 8
LANES = 128
BF = jnp.bfloat16
F32 = jnp.float32
DP = ("y", "x")
TP = ("z", "c")
VMEM = pl.BlockSpec(memory_space=pltpu.VMEM)
SMALL = pltpu.CompilerParams(vmem_limit_bytes=12 * 1024 * 1024)


def exchange(parts, axis):
    return lax.all_to_all(parts, axis, 0, 0, tiled=True)


def project_kernel(b, rows_ref, gain_ref, *refs):
    *weights, out_ref = refs
    groups, pad, width = rows_ref.shape
    rows = rows_ref[...].astype(F32).reshape(groups * pad, width)
    squares = jnp.sum(rows * rows, axis=1, keepdims=True)
    hidden = (rows * gain_ref[b : b + 1, :].astype(F32)).astype(BF)
    at = 0
    for w in weights:
        n = w.shape[2]
        part = jnp.dot(hidden, w[b], preferred_element_type=F32)
        out_ref[:, :, at : at + n] = part.reshape(groups, pad, n).astype(BF)
        at += n
    lane = lax.broadcasted_iota(jnp.int32, (groups * pad, LANES), 1)
    last = jnp.where(lane == 0, squares, 0.0)
    out_ref[:, :, at : at + LANES] = last.reshape(groups, pad, LANES).astype(BF)


def project(b, rows, gain, weights):
    cols = sum(w.shape[2] for w in weights) + LANES
    return pl.pallas_call(
        functools.partial(project_kernel, b),
        out_shape=jax.ShapeDtypeStruct((*rows.shape[:2], cols), BF),
        in_specs=[VMEM] * (2 + len(weights)),
        out_specs=VMEM,
        compiler_params=SMALL,
        name="project",
    )(rows, gain, *weights)


def spread_kernel(rows_ref, out_ref):
    rows = rows_ref[...].astype(F32)
    rows = jnp.concatenate([rows, jnp.zeros((PAD - rows.shape[0], rows.shape[1]), F32)], axis=0)
    out_ref[...] = jnp.broadcast_to(rows[None], out_ref.shape).astype(BF)


def spread(rows, n):
    return pl.pallas_call(
        spread_kernel,
        out_shape=jax.ShapeDtypeStruct((n, PAD, rows.shape[1]), BF),
        in_specs=[VMEM],
        out_specs=VMEM,
        compiler_params=SMALL,
        cost_estimate=pl.CostEstimate(flops=10**10, bytes_accessed=10**7, transcendentals=0),
        name="spread",
    )(rows)


def step_kernel(b, seqs, kc, vc, parts_ref, shift_ref, fade_ref, state_ref, out_ref, d_ref, k_ref, v_ref):
    total = jnp.sum(parts_ref[...].astype(F32), axis=0)
    cols = 3 * kc + 2 * vc
    total = total * lax.rsqrt(total[:, cols : cols + 1] / D + 1e-06)
    queries = total[:seqs, :kc] * DK ** (-0.5)
    keys = total[:seqs, kc : 2 * kc]
    pre = total[:seqs, 2 * kc : 3 * kc] + shift_ref[b : b + 1, :]
    values = total[:seqs, 3 * kc : 3 * kc + vc]
    gates = total[:seqs, 3 * kc + vc : cols]
    log_sigmoid = jnp.minimum(pre, 0.0) - jnp.log1p(jnp.exp(-jnp.abs(pre)))
    decay = jnp.exp(log_sigmoid / 16.0 + fade_ref[:, b, :])
    fresh_part = jnp.sum(queries * keys, axis=1, keepdims=True) * values
    columns = jnp.concatenate([queries * decay, jnp.zeros((PAD - seqs, kc), F32)], axis=0).T
    old = [
        jnp.sum(columns[:, s : s + 1] * state_ref[b, s], axis=0, keepdims=True) for s in range(seqs)
    ]
    readout = jnp.concatenate(old, axis=0) + fresh_part
    gated = readout * (gates / (1.0 + jnp.exp(-gates)))
    gated = jnp.concatenate([gated, jnp.zeros((PAD - seqs, vc), F32)], axis=0)
    out_ref[...] = jnp.broadcast_to(gated[None], out_ref.shape).astype(BF)
    d_ref[...] = decay
    k_ref[...] = keys
    v_ref[...] = values


def step(b, parts, shift, fade, state):
    seqs, _, kc = fade.shape
    vc = state.shape[3]
    return pl.pallas_call(
        functools.partial(step_kernel, b, seqs, kc, vc),
        out_shape=(
            jax.ShapeDtypeStruct((parts.shape[0], PAD, vc), BF),
            jax.ShapeDtypeStruct((seqs, kc), F32),
            jax.ShapeDtypeStruct((seqs, kc), F32),
            jax.ShapeDtypeStruct((seqs, vc), F32),
        ),
        in_specs=[VMEM] * 4,
        out_specs=(VMEM,) * 4,
        compiler_params=SMALL,
        name="step",
    )(parts, shift, fade, state)


def readback_kernel(b, gated_ref, weight_ref, out_ref):
    groups, pad, width = gated_ref.shape
    gated = gated_ref[...].astype(F32).reshape(groups * pad, width).astype(BF)
    branch = jnp.dot(gated, weight_ref[b], preferred_element_type=F32)
    out_ref[...] = branch.reshape(groups, pad, -1).astype(BF)


def readback(b, gated, weight):
    return pl.pallas_call(
        functools.partial(readback_kernel, b),
        out_shape=jax.ShapeDtypeStruct((*gated.shape[:2], weight.shape[2]), BF),
        in_specs=[VMEM] * 2,
        out_specs=VMEM,
        compiler_params=SMALL,
        name="readback",
    )(gated, weight)


def shards(
    incoming_embeddings,
    rescale_factors,
    probe_lift,
    address_lift,
    forget_lift,
    forget_shift,
    surplus_fade,
    content_lift,
    filter_lift,
    readback_lift,
    memory_tensor,
):
    weights = (probe_lift, address_lift, forget_lift, content_lift, filter_lift)
    depth = lax.axis_size("z")
    third = incoming_embeddings.shape[0]
    stream, first_core = lax.optimization_barrier((incoming_embeddings, lax.axis_index("c") == 0))
    stream = lax.all_gather(stream, "c", axis=0, tiled=True)
    fade = jnp.transpose(surplus_fade, (1, 0, 2))
    kept = []
    for b in range(BLOCKS):
        if b == 0:
            rows = exchange(spread(stream, depth), "z")
            stream = jnp.pad(stream, ((0, PAD - stream.shape[0]), (0, 0)))
        else:
            rows = exchange(jnp.broadcast_to(stream[None], (depth, *stream.shape)), "z")
        parts = exchange(project(b, rows, rescale_factors, weights), DP)
        gated, *small = step(b, parts, forget_shift, fade, memory_tensor)
        gathered = exchange(gated, DP)
        if b == BLOCKS - 1:
            kept.append(small)
            gathered, kept = lax.optimization_barrier((gathered, kept))
        else:
            kept.append(small)
        heads = exchange(readback(b, gathered, readback_lift), "z")
        own = jnp.sum(heads.astype(F32), axis=0)
        both = lax.all_gather(own, "c", axis=0)
        stream = (stream.astype(F32) + (both[0] + both[1])).astype(BF)
    fresh = [
        memory_tensor[b] * d[:, :, None] + k[:, :, None] * v[:, None, :]
        for b, (d, k, v) in enumerate(kept)
    ]
    mixed = jnp.where(first_core, stream[:third], stream[third : 2 * third])
    return mixed, jnp.stack(fresh)


def solution(mesh):
    z = mesh.shape["tp"] // 2
    fine = Mesh(mesh.devices.reshape(z, 2, 4, 4), ("z", "c", "y", "x"))
    in_specs = (
        P(TP, DP),
        P(None, DP),
        P(None, DP, TP),
        P(None, DP, TP),
        P(None, DP, TP),
        P(None, TP),
        P(None, DP, TP),
        P(None, DP, TP),
        P(None, DP, TP),
        P(None, TP, DP),
        P(None, DP, None, TP),
    )
    out_specs = (P(TP, DP), P(None, DP, None, TP))
    return jax.shard_map(shards, mesh=fine, in_specs=in_specs, out_specs=out_specs, check_vma=False)
```

```python
import functools

import jax
import jax.numpy as jnp
from jax import lax
from jax.experimental import pallas as pl
from jax.experimental.pallas import tpu as pltpu
from jax.sharding import Mesh, PartitionSpec as P

D = 4096
DK = 128
BLOCKS = 2
PAD = 8
LANES = 128
BF = jnp.bfloat16
F32 = jnp.float32
DP = ("y", "x")
TP = ("z", "c")
VMEM = pl.BlockSpec(memory_space=pltpu.VMEM)
SMALL = pltpu.CompilerParams(vmem_limit_bytes=12 * 1024 * 1024)


ORDER = {
    "z": tuple((8 + k) % 16 for k in range(16)),
    DP: tuple((10 + k) % 16 for k in range(16)),
}


def exchange(parts, axis):
    return lax.all_to_all(parts, axis, 0, 0, tiled=True, axis_index_groups=[list(ORDER[axis])])


def reordered(ref, source, target):
    at = [ORDER[source].index(i) for i in ORDER[target]]
    return jnp.concatenate([ref[i].astype(F32) for i in at], axis=0)


def project_kernel(b, rows_ref, gain_ref, *refs):
    *weights, out_ref = refs
    groups, pad, width = rows_ref.shape
    rows = reordered(rows_ref, "z", DP)
    squares = jnp.sum(rows * rows, axis=1, keepdims=True)
    hidden = (rows * gain_ref[b : b + 1, :].astype(F32)).astype(BF)
    at = 0
    for w in weights:
        n = w.shape[2]
        part = jnp.dot(hidden, w[b], preferred_element_type=F32)
        out_ref[:, :, at : at + n] = part.reshape(groups, pad, n).astype(BF)
        at += n
    lane = lax.broadcasted_iota(jnp.int32, (groups * pad, LANES), 1)
    last = jnp.where(lane == 0, squares, 0.0)
    out_ref[:, :, at : at + LANES] = last.reshape(groups, pad, LANES).astype(BF)


def project(b, rows, gain, weights):
    cols = sum(w.shape[2] for w in weights) + LANES
    return pl.pallas_call(
        functools.partial(project_kernel, b),
        out_shape=jax.ShapeDtypeStruct((*rows.shape[:2], cols), BF),
        in_specs=[VMEM] * (2 + len(weights)),
        out_specs=VMEM,
        compiler_params=SMALL,
        name="project",
    )(rows, gain, *weights)


def spread_kernel(rows_ref, out_ref):
    rows = rows_ref[...].astype(F32)
    rows = jnp.concatenate([rows, jnp.zeros((PAD - rows.shape[0], rows.shape[1]), F32)], axis=0)
    out_ref[...] = jnp.broadcast_to(rows[None], out_ref.shape).astype(BF)


def spread(rows, n):
    return pl.pallas_call(
        spread_kernel,
        out_shape=jax.ShapeDtypeStruct((n, PAD, rows.shape[1]), BF),
        in_specs=[VMEM],
        out_specs=VMEM,
        compiler_params=SMALL,
        cost_estimate=pl.CostEstimate(flops=10**10, bytes_accessed=10**7, transcendentals=0),
        name="spread",
    )(rows)


def step_kernel(b, seqs, kc, vc, parts_ref, shift_ref, fade_ref, state_ref, out_ref, d_ref, k_ref, v_ref):
    total = jnp.sum(parts_ref[...].astype(F32), axis=0)
    cols = 3 * kc + 2 * vc
    total = total * lax.rsqrt(total[:, cols : cols + 1] / D + 1e-06)
    queries = total[:seqs, :kc] * DK ** (-0.5)
    keys = total[:seqs, kc : 2 * kc]
    pre = total[:seqs, 2 * kc : 3 * kc] + shift_ref[b : b + 1, :]
    values = total[:seqs, 3 * kc : 3 * kc + vc]
    gates = total[:seqs, 3 * kc + vc : cols]
    log_sigmoid = jnp.minimum(pre, 0.0) - jnp.log1p(jnp.exp(-jnp.abs(pre)))
    decay = jnp.exp(log_sigmoid / 16.0 + fade_ref[:, b, :])
    fresh_part = jnp.sum(queries * keys, axis=1, keepdims=True) * values
    columns = jnp.concatenate([queries * decay, jnp.zeros((PAD - seqs, kc), F32)], axis=0).T
    old = [
        jnp.sum(columns[:, s : s + 1] * state_ref[b, s], axis=0, keepdims=True) for s in range(seqs)
    ]
    readout = jnp.concatenate(old, axis=0) + fresh_part
    gated = readout * (gates / (1.0 + jnp.exp(-gates)))
    gated = jnp.concatenate([gated, jnp.zeros((PAD - seqs, vc), F32)], axis=0)
    out_ref[...] = jnp.broadcast_to(gated[None], out_ref.shape).astype(BF)
    d_ref[...] = decay
    k_ref[...] = keys
    v_ref[...] = values


def step(b, parts, shift, fade, state):
    seqs, _, kc = fade.shape
    vc = state.shape[3]
    return pl.pallas_call(
        functools.partial(step_kernel, b, seqs, kc, vc),
        out_shape=(
            jax.ShapeDtypeStruct((parts.shape[0], PAD, vc), BF),
            jax.ShapeDtypeStruct((seqs, kc), F32),
            jax.ShapeDtypeStruct((seqs, kc), F32),
            jax.ShapeDtypeStruct((seqs, vc), F32),
        ),
        in_specs=[VMEM] * 4,
        out_specs=(VMEM,) * 4,
        compiler_params=SMALL,
        name="step",
    )(parts, shift, fade, state)


def readback_kernel(b, gated_ref, weight_ref, out_ref):
    groups, pad, width = gated_ref.shape
    gated = reordered(gated_ref, DP, "z").astype(BF)
    branch = jnp.dot(gated, weight_ref[b], preferred_element_type=F32)
    out_ref[...] = branch.reshape(groups, pad, -1).astype(BF)


def readback(b, gated, weight):
    return pl.pallas_call(
        functools.partial(readback_kernel, b),
        out_shape=jax.ShapeDtypeStruct((*gated.shape[:2], weight.shape[2]), BF),
        in_specs=[VMEM] * 2,
        out_specs=VMEM,
        compiler_params=SMALL,
        name="readback",
    )(gated, weight)


def shards(
    incoming_embeddings,
    rescale_factors,
    probe_lift,
    address_lift,
    forget_lift,
    forget_shift,
    surplus_fade,
    content_lift,
    filter_lift,
    readback_lift,
    memory_tensor,
):
    weights = (probe_lift, address_lift, forget_lift, content_lift, filter_lift)
    depth = lax.axis_size("z")
    third = incoming_embeddings.shape[0]
    stream, first_core = lax.optimization_barrier((incoming_embeddings, lax.axis_index("c") == 0))
    stream = lax.all_gather(stream, "c", axis=0, tiled=True)
    fade = jnp.transpose(surplus_fade, (1, 0, 2))
    kept = []
    for b in range(BLOCKS):
        if b == 0:
            rows = exchange(spread(stream, depth), "z")
            stream = jnp.pad(stream, ((0, PAD - stream.shape[0]), (0, 0)))
        else:
            rows = exchange(jnp.broadcast_to(stream[None], (depth, *stream.shape)), "z")
        parts = exchange(project(b, rows, rescale_factors, weights), DP)
        gated, *small = step(b, parts, forget_shift, fade, memory_tensor)
        gathered = exchange(gated, DP)
        if b == BLOCKS - 1:
            kept.append(small)
            gathered, kept = lax.optimization_barrier((gathered, kept))
        else:
            kept.append(small)
        heads = exchange(readback(b, gathered, readback_lift), "z")
        own = jnp.sum(heads.astype(F32), axis=0)
        both = lax.all_gather(own, "c", axis=0)
        stream = (stream.astype(F32) + (both[0] + both[1])).astype(BF)
    fresh = [
        memory_tensor[b] * d[:, :, None] + k[:, :, None] * v[:, None, :]
        for b, (d, k, v) in enumerate(kept)
    ]
    mixed = jnp.where(first_core, stream[:third], stream[third : 2 * third])
    return mixed, jnp.stack(fresh)


def solution(mesh):
    z = mesh.shape["tp"] // 2
    fine = Mesh(mesh.devices.reshape(z, 2, 4, 4), ("z", "c", "y", "x"))
    in_specs = (
        P(TP, DP),
        P(None, DP),
        P(None, DP, TP),
        P(None, DP, TP),
        P(None, DP, TP),
        P(None, TP),
        P(None, DP, TP),
        P(None, DP, TP),
        P(None, DP, TP),
        P(None, TP, DP),
        P(None, DP, None, TP),
    )
    out_specs = (P(TP, DP), P(None, DP, None, TP))
    return jax.shard_map(shards, mesh=fine, in_specs=in_specs, out_specs=out_specs, check_vma=False)
```

```python
import functools

import jax
import jax.numpy as jnp
from jax import lax
from jax.experimental import pallas as pl
from jax.experimental.pallas import tpu as pltpu
from jax.sharding import Mesh, PartitionSpec as P

D = 4096
DK = 128
BLOCKS = 2
PAD = 8
LANES = 128
BF = jnp.bfloat16
F32 = jnp.float32
DP = ("y", "x")
TP = ("z", "c")
VMEM = pl.BlockSpec(memory_space=pltpu.VMEM)
SMALL = pltpu.CompilerParams(vmem_limit_bytes=12 * 1024 * 1024)


ORDER = {
    "z": tuple((8 + k) % 16 for k in range(16)),
    DP: tuple((10 + k) % 16 for k in range(16)),
}
ORDER[TP] = tuple(2 * z + c for z in ORDER["z"] for c in (1, 0))
HALF = PAD // 2


def exchange(parts, axis):
    return lax.all_to_all(parts, axis, 0, 0, tiled=True, axis_index_groups=[list(ORDER[axis])])


def reordered(ref, source, target):
    at = [ORDER[source].index(i) for i in ORDER[target]]
    return jnp.concatenate([ref[i].astype(F32) for i in at], axis=0)


def project_kernel(b, rows_ref, gain_ref, *refs):
    *weights, out_ref = refs
    groups, pad, width = rows_ref.shape
    rows = reordered(rows_ref, "z", DP)
    squares = jnp.sum(rows * rows, axis=1, keepdims=True)
    hidden = (rows * gain_ref[b : b + 1, :].astype(F32)).astype(BF)
    at = 0
    for w in weights:
        n = w.shape[2]
        part = jnp.dot(hidden, w[b], preferred_element_type=F32)
        out_ref[:, :, at : at + n] = part.reshape(groups, pad, n).astype(BF)
        at += n
    lane = lax.broadcasted_iota(jnp.int32, (groups * pad, LANES), 1)
    last = jnp.where(lane == 0, squares, 0.0)
    out_ref[:, :, at : at + LANES] = last.reshape(groups, pad, LANES).astype(BF)


def project(b, rows, gain, weights):
    cols = sum(w.shape[2] for w in weights) + LANES
    return pl.pallas_call(
        functools.partial(project_kernel, b),
        out_shape=jax.ShapeDtypeStruct((*rows.shape[:2], cols), BF),
        in_specs=[VMEM] * (2 + len(weights)),
        out_specs=VMEM,
        compiler_params=SMALL,
        name="project",
    )(rows, gain, *weights)


def spread_kernel(rows_ref, out_ref):
    rows = rows_ref[...].astype(F32)
    rows = jnp.concatenate([rows, jnp.zeros((HALF - rows.shape[0], rows.shape[1]), F32)], axis=0)
    out_ref[...] = jnp.broadcast_to(rows[None], out_ref.shape).astype(BF)


def spread(rows, n):
    return pl.pallas_call(
        spread_kernel,
        out_shape=jax.ShapeDtypeStruct((n, HALF, rows.shape[1]), BF),
        in_specs=[VMEM],
        out_specs=VMEM,
        compiler_params=SMALL,
        cost_estimate=pl.CostEstimate(flops=10**10, bytes_accessed=10**7, transcendentals=0),
        name="spread",
    )(rows)


def step_kernel(b, seqs, kc, vc, parts_ref, shift_ref, fade_ref, state_ref, out_ref, d_ref, k_ref, v_ref):
    total = jnp.sum(parts_ref[...].astype(F32), axis=0)
    third = seqs // 2
    total = jnp.concatenate([total[HALF : HALF + third], total[:third]], axis=0)
    cols = 3 * kc + 2 * vc
    total = total * lax.rsqrt(total[:, cols : cols + 1] / D + 1e-06)
    queries = total[:, :kc] * DK ** (-0.5)
    keys = total[:, kc : 2 * kc]
    pre = total[:, 2 * kc : 3 * kc] + shift_ref[b : b + 1, :]
    values = total[:, 3 * kc : 3 * kc + vc]
    gates = total[:, 3 * kc + vc : cols]
    log_sigmoid = jnp.minimum(pre, 0.0) - jnp.log1p(jnp.exp(-jnp.abs(pre)))
    decay = jnp.exp(log_sigmoid / 16.0 + fade_ref[:, b, :])
    fresh_part = jnp.sum(queries * keys, axis=1, keepdims=True) * values
    columns = jnp.concatenate([queries * decay, jnp.zeros((PAD - seqs, kc), F32)], axis=0).T
    old = [
        jnp.sum(columns[:, s : s + 1] * state_ref[b, s], axis=0, keepdims=True) for s in range(seqs)
    ]
    readout = jnp.concatenate(old, axis=0) + fresh_part
    gated = readout * (gates / (1.0 + jnp.exp(-gates)))
    blank = jnp.zeros((HALF - third, vc), F32)
    gated = jnp.concatenate([gated[third:], blank, gated[:third], blank], axis=0)
    out_ref[...] = jnp.broadcast_to(gated[None], out_ref.shape).astype(BF)
    d_ref[...] = decay
    k_ref[...] = keys
    v_ref[...] = values


def step(b, parts, shift, fade, state):
    seqs, _, kc = fade.shape
    vc = state.shape[3]
    return pl.pallas_call(
        functools.partial(step_kernel, b, seqs, kc, vc),
        out_shape=(
            jax.ShapeDtypeStruct((parts.shape[0], PAD, vc), BF),
            jax.ShapeDtypeStruct((seqs, kc), F32),
            jax.ShapeDtypeStruct((seqs, kc), F32),
            jax.ShapeDtypeStruct((seqs, vc), F32),
        ),
        in_specs=[VMEM] * 4,
        out_specs=(VMEM,) * 4,
        compiler_params=SMALL,
        name="step",
    )(parts, shift, fade, state)


def readback_kernel(b, gated_ref, weight_ref, out_ref):
    groups, pad, width = gated_ref.shape
    gated = reordered(gated_ref, DP, "z").astype(BF)
    branch = jnp.dot(gated, weight_ref[b], preferred_element_type=F32)
    out_ref[...] = branch.reshape(groups, pad, -1).astype(BF)


def readback(b, gated, weight):
    return pl.pallas_call(
        functools.partial(readback_kernel, b),
        out_shape=jax.ShapeDtypeStruct((*gated.shape[:2], weight.shape[2]), BF),
        in_specs=[VMEM] * 2,
        out_specs=VMEM,
        compiler_params=SMALL,
        name="readback",
    )(gated, weight)


def shards(
    incoming_embeddings,
    rescale_factors,
    probe_lift,
    address_lift,
    forget_lift,
    forget_shift,
    surplus_fade,
    content_lift,
    filter_lift,
    readback_lift,
    memory_tensor,
):
    weights = (probe_lift, address_lift, forget_lift, content_lift, filter_lift)
    depth = lax.axis_size("z")
    third, width = incoming_embeddings.shape
    place = lax.rem(lax.axis_index("z") + depth - ORDER["z"][0], depth).astype(jnp.uint32)
    stream, north, place = lax.optimization_barrier(
        (incoming_embeddings, lax.axis_index("c") == 1, place)
    )
    fade = jnp.transpose(surplus_fade, (1, 0, 2))
    kept = []
    for b in range(BLOCKS):
        if b == 0:
            rows = exchange(spread(stream, 2 * depth), TP).reshape(depth, PAD, width)
            old = lax.dynamic_index_in_dim(rows, place, 0, keepdims=False)
            rows, old = lax.optimization_barrier((rows, old))
        else:
            rows = exchange(jnp.broadcast_to(stream[None], (depth, *stream.shape)), "z")
        parts = exchange(project(b, rows, rescale_factors, weights), DP)
        gated, *small = step(b, parts, forget_shift, fade, memory_tensor)
        kept.append(small)
        gathered = exchange(gated, DP)
        if b == 0:
            heads = exchange(readback(b, gathered, readback_lift), "z")
            own = jnp.sum(heads.astype(F32), axis=0)
            both = lax.all_gather(own, "c", axis=0)
            stream = (old.astype(F32) + (both[0] + both[1])).astype(BF)
            rest = jnp.where(north, stream[:third], stream[HALF : HALF + third]).astype(F32)
            stream, rest = lax.optimization_barrier((stream, rest))
        else:
            gathered, kept, rest = lax.optimization_barrier((gathered, kept, rest))
            parts = readback(b, gathered, readback_lift).reshape(2 * depth, HALF, width)
            branch = jnp.sum(exchange(parts, TP).astype(F32), axis=0)[:third]
            mixed = (rest + branch).astype(BF)
    fresh = [
        memory_tensor[b] * d[:, :, None] + k[:, :, None] * v[:, None, :]
        for b, (d, k, v) in enumerate(kept)
    ]
    return mixed, jnp.stack(fresh)


def solution(mesh):
    z = mesh.shape["tp"] // 2
    fine = Mesh(mesh.devices.reshape(z, 2, 4, 4), ("z", "c", "y", "x"))
    in_specs = (
        P(TP, DP),
        P(None, DP),
        P(None, DP, TP),
        P(None, DP, TP),
        P(None, DP, TP),
        P(None, TP),
        P(None, DP, TP),
        P(None, DP, TP),
        P(None, DP, TP),
        P(None, TP, DP),
        P(None, DP, None, TP),
    )
    out_specs = (P(TP, DP), P(None, DP, None, TP))
    return jax.shard_map(shards, mesh=fine, in_specs=in_specs, out_specs=out_specs, check_vma=False)
```

```python
import functools

import jax
import jax.numpy as jnp
from jax import lax
from jax.experimental import pallas as pl
from jax.experimental.pallas import tpu as pltpu
from jax.sharding import Mesh, PartitionSpec as P

D = 4096
DK = 128
BLOCKS = 2
PAD = 8
LANES = 128
BF = jnp.bfloat16
F32 = jnp.float32
DP = ("y", "x")
TP = ("z", "c")
VMEM = pl.BlockSpec(memory_space=pltpu.VMEM)
SMALL = pltpu.CompilerParams(vmem_limit_bytes=12 * 1024 * 1024)


ORDER = {
    "z": tuple((8 + k) % 16 for k in range(16)),
    DP: tuple((10 + k) % 16 for k in range(16)),
}
ORDER[TP] = tuple(2 * z + c for z in ORDER["z"] for c in (1, 0))
HALF = PAD // 2


def exchange(parts, axis):
    return lax.all_to_all(parts, axis, 0, 0, tiled=True, axis_index_groups=[list(ORDER[axis])])


def reordered(ref, source, target):
    at = [ORDER[source].index(i) for i in ORDER[target]]
    return jnp.concatenate([ref[i].astype(F32) for i in at], axis=0)


def project_kernel(b, rows_ref, gain_ref, *refs):
    *weights, out_ref = refs
    groups, pad, width = rows_ref.shape
    rows = reordered(rows_ref, "z", DP)
    squares = jnp.sum(rows * rows, axis=1, keepdims=True)
    hidden = (rows * gain_ref[b : b + 1, :].astype(F32)).astype(BF)
    at = 0
    for w in weights:
        n = w.shape[2]
        part = jnp.dot(hidden, w[b], preferred_element_type=F32)
        out_ref[:, :, at : at + n] = part.reshape(groups, pad, n).astype(BF)
        at += n
    lane = lax.broadcasted_iota(jnp.int32, (groups * pad, LANES), 1)
    last = jnp.where(lane == 0, squares, 0.0)
    out_ref[:, :, at : at + LANES] = last.reshape(groups, pad, LANES).astype(BF)


def project(b, rows, gain, weights):
    cols = sum(w.shape[2] for w in weights) + LANES
    return pl.pallas_call(
        functools.partial(project_kernel, b),
        out_shape=jax.ShapeDtypeStruct((*rows.shape[:2], cols), BF),
        in_specs=[VMEM] * (2 + len(weights)),
        out_specs=VMEM,
        compiler_params=SMALL,
        name="project",
    )(rows, gain, *weights)


def spread_kernel(rows_ref, out_ref):
    rows = rows_ref[...].astype(F32)
    rows = jnp.concatenate([rows, jnp.zeros((HALF - rows.shape[0], rows.shape[1]), F32)], axis=0)
    out_ref[...] = jnp.broadcast_to(rows[None], out_ref.shape).astype(BF)


def spread(rows, n):
    return pl.pallas_call(
        spread_kernel,
        out_shape=jax.ShapeDtypeStruct((n, HALF, rows.shape[1]), BF),
        in_specs=[VMEM],
        out_specs=VMEM,
        compiler_params=SMALL,
        cost_estimate=pl.CostEstimate(flops=10**10, bytes_accessed=10**7, transcendentals=0),
        name="spread",
    )(rows)


def step_kernel(b, seqs, kc, vc, parts_ref, shift_ref, fade_ref, state_ref, out_ref, d_ref, k_ref, v_ref):
    total = jnp.sum(parts_ref[...].astype(F32), axis=0)
    third = seqs // 2
    total = jnp.concatenate([total[HALF : HALF + third], total[:third]], axis=0)
    cols = 3 * kc + 2 * vc
    total = total * lax.rsqrt(total[:, cols : cols + 1] / D + 1e-06)
    queries = total[:, :kc] * DK ** (-0.5)
    keys = total[:, kc : 2 * kc]
    pre = total[:, 2 * kc : 3 * kc] + shift_ref[b : b + 1, :]
    values = total[:, 3 * kc : 3 * kc + vc]
    gates = total[:, 3 * kc + vc : cols]
    log_sigmoid = jnp.minimum(pre, 0.0) - jnp.log1p(jnp.exp(-jnp.abs(pre)))
    decay = jnp.exp(log_sigmoid / 16.0 + fade_ref[:, b, :])
    fresh_part = jnp.sum(queries * keys, axis=1, keepdims=True) * values
    columns = jnp.concatenate([queries * decay, jnp.zeros((PAD - seqs, kc), F32)], axis=0).T
    old = [
        jnp.sum(columns[:, s : s + 1] * state_ref[b, s], axis=0, keepdims=True) for s in range(seqs)
    ]
    readout = jnp.concatenate(old, axis=0) + fresh_part
    gated = readout * (gates / (1.0 + jnp.exp(-gates)))
    blank = jnp.zeros((HALF - third, vc), F32)
    gated = jnp.concatenate([gated[third:], blank, gated[:third], blank], axis=0)
    out_ref[...] = jnp.broadcast_to(gated[None], out_ref.shape).astype(BF)
    d_ref[...] = decay
    k_ref[...] = keys
    v_ref[...] = values


def step(b, parts, shift, fade, state):
    seqs, _, kc = fade.shape
    vc = state.shape[3]
    return pl.pallas_call(
        functools.partial(step_kernel, b, seqs, kc, vc),
        out_shape=(
            jax.ShapeDtypeStruct((parts.shape[0], PAD, vc), BF),
            jax.ShapeDtypeStruct((seqs, kc), F32),
            jax.ShapeDtypeStruct((seqs, kc), F32),
            jax.ShapeDtypeStruct((seqs, vc), F32),
        ),
        in_specs=[VMEM] * 4,
        out_specs=(VMEM,) * 4,
        compiler_params=SMALL,
        name="step",
    )(parts, shift, fade, state)


def readback_kernel(b, gated_ref, weight_ref, out_ref):
    groups, pad, width = gated_ref.shape
    gated = reordered(gated_ref, DP, "z").astype(BF)
    branch = jnp.dot(gated, weight_ref[b], preferred_element_type=F32)
    out_ref[...] = branch.reshape(groups, pad, -1).astype(BF)


def readback(b, gated, weight):
    return pl.pallas_call(
        functools.partial(readback_kernel, b),
        out_shape=jax.ShapeDtypeStruct((*gated.shape[:2], weight.shape[2]), BF),
        in_specs=[VMEM] * 2,
        out_specs=VMEM,
        compiler_params=SMALL,
        name="readback",
    )(gated, weight)


def shards(
    incoming_embeddings,
    rescale_factors,
    probe_lift,
    address_lift,
    forget_lift,
    forget_shift,
    surplus_fade,
    content_lift,
    filter_lift,
    readback_lift,
    memory_tensor,
):
    weights = (probe_lift, address_lift, forget_lift, content_lift, filter_lift)
    depth = lax.axis_size("z")
    third, width = incoming_embeddings.shape
    fade = jnp.transpose(surplus_fade, (1, 0, 2))
    stream = incoming_embeddings
    kept = []
    for b in range(BLOCKS):
        if b == 0:
            copies = spread(stream, 2 * depth)
        else:
            copies = jnp.broadcast_to(
                jnp.pad(stream, ((0, HALF - third), (0, 0)))[None], (2 * depth, HALF, width)
            )
        rows = exchange(copies, TP).reshape(depth, PAD, width)
        parts = exchange(project(b, rows, rescale_factors, weights), DP)
        gated, *small = step(b, parts, forget_shift, fade, memory_tensor)
        kept.append(small)
        gathered = exchange(gated, DP)
        if b == BLOCKS - 1:
            gathered, kept = lax.optimization_barrier((gathered, kept))
        heads = readback(b, gathered, readback_lift).reshape(2 * depth, HALF, width)
        branch = jnp.sum(exchange(heads, TP).astype(F32), axis=0)[:third]
        stream = (stream.astype(F32) + branch).astype(BF)
    fresh = [
        memory_tensor[b] * d[:, :, None] + k[:, :, None] * v[:, None, :]
        for b, (d, k, v) in enumerate(kept)
    ]
    return stream, jnp.stack(fresh)


def solution(mesh):
    z = mesh.shape["tp"] // 2
    fine = Mesh(mesh.devices.reshape(z, 2, 4, 4), ("z", "c", "y", "x"))
    in_specs = (
        P(TP, DP),
        P(None, DP),
        P(None, DP, TP),
        P(None, DP, TP),
        P(None, DP, TP),
        P(None, TP),
        P(None, DP, TP),
        P(None, DP, TP),
        P(None, DP, TP),
        P(None, TP, DP),
        P(None, DP, None, TP),
    )
    out_specs = (P(TP, DP), P(None, DP, None, TP))
    return jax.shard_map(shards, mesh=fine, in_specs=in_specs, out_specs=out_specs, check_vma=False)
```

```python
import functools

import jax
import jax.numpy as jnp
from jax import lax
from jax.experimental import pallas as pl
from jax.experimental.pallas import tpu as pltpu
from jax.sharding import Mesh, PartitionSpec as P

D = 4096
DK = 128
BLOCKS = 2
PAD = 8
LANES = 128
BF = jnp.bfloat16
F32 = jnp.float32
DP = ("y", "x")
TP = ("z", "c")
VMEM = pl.BlockSpec(memory_space=pltpu.VMEM)
SMALL = pltpu.CompilerParams(vmem_limit_bytes=12 * 1024 * 1024)


ORDER = {
    "z": (8, 0, 9, 1, 10, 2, 11, 3, 12, 4, 13, 5, 14, 6, 15, 7),
    DP: (10, 0, 11, 1, 8, 2, 9, 3, 14, 4, 15, 5, 12, 6, 13, 7),
}
ORDER[TP] = tuple(2 * z + c for z in ORDER["z"] for c in (1, 0))
HALF = PAD // 2


def exchange(parts, axis):
    return lax.all_to_all(parts, axis, 0, 0, tiled=True, axis_index_groups=[list(ORDER[axis])])


def reordered(ref, source, target):
    at = [ORDER[source].index(i) for i in ORDER[target]]
    return jnp.concatenate([ref[i].astype(F32) for i in at], axis=0)


def project_kernel(b, rows_ref, gain_ref, *refs):
    *weights, out_ref = refs
    groups, pad, width = rows_ref.shape
    rows = reordered(rows_ref, "z", DP)
    squares = jnp.sum(rows * rows, axis=1, keepdims=True)
    hidden = (rows * gain_ref[b : b + 1, :].astype(F32)).astype(BF)
    at = 0
    for w in weights:
        n = w.shape[2]
        part = jnp.dot(hidden, w[b], preferred_element_type=F32)
        out_ref[:, :, at : at + n] = part.reshape(groups, pad, n).astype(BF)
        at += n
    lane = lax.broadcasted_iota(jnp.int32, (groups * pad, LANES), 1)
    last = jnp.where(lane == 0, squares, 0.0)
    out_ref[:, :, at : at + LANES] = last.reshape(groups, pad, LANES).astype(BF)


def project(b, rows, gain, weights):
    cols = sum(w.shape[2] for w in weights) + LANES
    return pl.pallas_call(
        functools.partial(project_kernel, b),
        out_shape=jax.ShapeDtypeStruct((*rows.shape[:2], cols), BF),
        in_specs=[VMEM] * (2 + len(weights)),
        out_specs=VMEM,
        compiler_params=SMALL,
        name="project",
    )(rows, gain, *weights)


def spread_kernel(rows_ref, out_ref):
    rows = rows_ref[...].astype(F32)
    rows = jnp.concatenate([rows, jnp.zeros((HALF - rows.shape[0], rows.shape[1]), F32)], axis=0)
    out_ref[...] = jnp.broadcast_to(rows[None], out_ref.shape).astype(BF)


def spread(rows, n):
    return pl.pallas_call(
        spread_kernel,
        out_shape=jax.ShapeDtypeStruct((n, HALF, rows.shape[1]), BF),
        in_specs=[VMEM],
        out_specs=VMEM,
        compiler_params=SMALL,
        cost_estimate=pl.CostEstimate(flops=10**10, bytes_accessed=10**7, transcendentals=0),
        name="spread",
    )(rows)


def step_kernel(b, seqs, kc, vc, parts_ref, shift_ref, fade_ref, state_ref, out_ref, d_ref, k_ref, v_ref):
    total = jnp.sum(parts_ref[...].astype(F32), axis=0)
    third = seqs // 2
    total = jnp.concatenate([total[HALF : HALF + third], total[:third]], axis=0)
    cols = 3 * kc + 2 * vc
    total = total * lax.rsqrt(total[:, cols : cols + 1] / D + 1e-06)
    queries = total[:, :kc] * DK ** (-0.5)
    keys = total[:, kc : 2 * kc]
    pre = total[:, 2 * kc : 3 * kc] + shift_ref[b : b + 1, :]
    values = total[:, 3 * kc : 3 * kc + vc]
    gates = total[:, 3 * kc + vc : cols]
    log_sigmoid = jnp.minimum(pre, 0.0) - jnp.log1p(jnp.exp(-jnp.abs(pre)))
    decay = jnp.exp(log_sigmoid / 16.0 + fade_ref[:, b, :])
    fresh_part = jnp.sum(queries * keys, axis=1, keepdims=True) * values
    columns = jnp.concatenate([queries * decay, jnp.zeros((PAD - seqs, kc), F32)], axis=0).T
    old = [
        jnp.sum(columns[:, s : s + 1] * state_ref[b, s], axis=0, keepdims=True) for s in range(seqs)
    ]
    readout = jnp.concatenate(old, axis=0) + fresh_part
    gated = readout * (gates / (1.0 + jnp.exp(-gates)))
    blank = jnp.zeros((HALF - third, vc), F32)
    gated = jnp.concatenate([gated[third:], blank, gated[:third], blank], axis=0)
    out_ref[...] = jnp.broadcast_to(gated[None], out_ref.shape).astype(BF)
    d_ref[...] = decay
    k_ref[...] = keys
    v_ref[...] = values


def step(b, parts, shift, fade, state):
    seqs, _, kc = fade.shape
    vc = state.shape[3]
    return pl.pallas_call(
        functools.partial(step_kernel, b, seqs, kc, vc),
        out_shape=(
            jax.ShapeDtypeStruct((parts.shape[0], PAD, vc), BF),
            jax.ShapeDtypeStruct((seqs, kc), F32),
            jax.ShapeDtypeStruct((seqs, kc), F32),
            jax.ShapeDtypeStruct((seqs, vc), F32),
        ),
        in_specs=[VMEM] * 4,
        out_specs=(VMEM,) * 4,
        compiler_params=SMALL,
        name="step",
    )(parts, shift, fade, state)


def readback_kernel(b, gated_ref, weight_ref, out_ref):
    groups, pad, width = gated_ref.shape
    gated = reordered(gated_ref, DP, "z").astype(BF)
    branch = jnp.dot(gated, weight_ref[b], preferred_element_type=F32)
    out_ref[...] = branch.reshape(groups, pad, -1).astype(BF)


def readback(b, gated, weight):
    return pl.pallas_call(
        functools.partial(readback_kernel, b),
        out_shape=jax.ShapeDtypeStruct((*gated.shape[:2], weight.shape[2]), BF),
        in_specs=[VMEM] * 2,
        out_specs=VMEM,
        compiler_params=SMALL,
        name="readback",
    )(gated, weight)


def shards(
    incoming_embeddings,
    rescale_factors,
    probe_lift,
    address_lift,
    forget_lift,
    forget_shift,
    surplus_fade,
    content_lift,
    filter_lift,
    readback_lift,
    memory_tensor,
):
    weights = (probe_lift, address_lift, forget_lift, content_lift, filter_lift)
    depth = lax.axis_size("z")
    third, width = incoming_embeddings.shape
    fade = jnp.transpose(surplus_fade, (1, 0, 2))
    stream = incoming_embeddings
    kept = []
    for b in range(BLOCKS):
        if b == 0:
            copies = spread(stream, 2 * depth)
        else:
            copies = jnp.broadcast_to(
                jnp.pad(stream, ((0, HALF - third), (0, 0)))[None], (2 * depth, HALF, width)
            )
        rows = exchange(copies, TP).reshape(depth, PAD, width)
        parts = exchange(project(b, rows, rescale_factors, weights), DP)
        gated, *small = step(b, parts, forget_shift, fade, memory_tensor)
        kept.append(small)
        gathered = exchange(gated, DP)
        if b == BLOCKS - 1:
            gathered, kept = lax.optimization_barrier((gathered, kept))
        heads = readback(b, gathered, readback_lift).reshape(2 * depth, HALF, width)
        branch = jnp.sum(exchange(heads, TP).astype(F32), axis=0)[:third]
        stream = (stream.astype(F32) + branch).astype(BF)
    fresh = [
        memory_tensor[b] * d[:, :, None] + k[:, :, None] * v[:, None, :]
        for b, (d, k, v) in enumerate(kept)
    ]
    return stream, jnp.stack(fresh)


def solution(mesh):
    z = mesh.shape["tp"] // 2
    fine = Mesh(mesh.devices.reshape(z, 2, 4, 4), ("z", "c", "y", "x"))
    in_specs = (
        P(TP, DP),
        P(None, DP),
        P(None, DP, TP),
        P(None, DP, TP),
        P(None, DP, TP),
        P(None, TP),
        P(None, DP, TP),
        P(None, DP, TP),
        P(None, DP, TP),
        P(None, TP, DP),
        P(None, DP, None, TP),
    )
    out_specs = (P(TP, DP), P(None, DP, None, TP))
    return jax.shard_map(shards, mesh=fine, in_specs=in_specs, out_specs=out_specs, check_vma=False)
```

```python
import functools

import jax
import jax.numpy as jnp
from jax import lax
from jax.experimental import pallas as pl
from jax.experimental.pallas import tpu as pltpu
from jax.sharding import Mesh, PartitionSpec as P

D = 4096
DK = 128
BLOCKS = 2
PAD = 8
LANES = 128
BF = jnp.bfloat16
F32 = jnp.float32
DP = ("y", "x")
TP = ("z", "c")
VMEM = pl.BlockSpec(memory_space=pltpu.VMEM)
SMALL = pltpu.CompilerParams(vmem_limit_bytes=12 * 1024 * 1024)


ORDER = {
    "z": tuple((8 + k) % 16 for k in range(16)),
    DP: tuple((10 + k) % 16 for k in range(16)),
}
ORDER[TP] = tuple(2 * z + c for z in ORDER["z"] for c in (1, 0))
SEQ_OF_ROW = (3, 0, 4, 1, 5, 2)


def exchange(parts, axis):
    return lax.all_to_all(parts, axis, 0, 0, tiled=True, axis_index_groups=[list(ORDER[axis])])


def shift_between():
    return (ORDER[DP][0] - ORDER["z"][0]) % len(ORDER["z"])


def project_kernel(b, pieces_ref, gain_ref, *refs):
    *weights, out_ref = refs
    groups = pieces_ref.shape[0] // 2
    pieces = pieces_ref[...].astype(F32)
    first, second = pieces[:, 0, :], pieces[:, 1, :]
    at = 2 * LANES
    mixed = jnp.concatenate([first[:, at:], second[:, :LANES]], axis=1)
    rows = jnp.concatenate([first[:, :at], mixed, second[:, LANES:]], axis=0).astype(BF)
    i = lax.broadcasted_iota(jnp.int32, (groups * PAD, rows.shape[0]), 0)
    column = lax.broadcasted_iota(jnp.int32, (groups * PAD, rows.shape[0]), 1)
    piece = 2 * (((i >> 3) + shift_between()) & (groups - 1)) + (i & 1)
    chosen = jnp.where(column == ((i & 7) >> 1) * 2 * groups + piece, 1.0, 0.0).astype(BF)
    rows = jnp.dot(chosen, rows, preferred_element_type=F32)
    squares = jnp.sum(rows * rows, axis=1, keepdims=True)
    hidden = (rows * gain_ref[b : b + 1, :].astype(F32)).astype(BF)
    tiles = []
    for w in weights:
        part = jnp.dot(hidden, w[b], preferred_element_type=F32)
        tiles += [part[:, k : k + LANES] for k in range(0, part.shape[1], LANES)]
    last = tiles.pop()
    row = lax.broadcasted_iota(jnp.int32, last.shape, 0) & 7
    lane = lax.broadcasted_iota(jnp.int32, last.shape, 1)
    spread_squares = jnp.broadcast_to(squares, last.shape)
    moved = [pltpu.roll(spread_squares, k, 0) for k in (6, 4, 2)]
    extra = [pltpu.roll(last, k, 0) for k in (6, 4, 2)]
    extra.append(jnp.where(lane == 0, moved[0], jnp.where(lane == 1, moved[1], moved[2])))
    for k, tile in enumerate(tiles):
        if k < len(extra):
            tile = jnp.where(row >= 6, extra[k], tile)
        out_ref[:, :, k * LANES : (k + 1) * LANES] = tile.reshape(groups, PAD, LANES).astype(BF)


def project(b, pieces, gain, weights):
    cols = sum(w.shape[2] for w in weights) - LANES
    return pl.pallas_call(
        functools.partial(project_kernel, b),
        out_shape=jax.ShapeDtypeStruct((pieces.shape[0] // 2, PAD, cols), BF),
        in_specs=[VMEM] * (2 + len(weights)),
        out_specs=VMEM,
        compiler_params=SMALL,
        name="project",
    )(pieces, gain, *weights)


def spread_kernel(rows_ref, out_ref, own_ref):
    rows = rows_ref[...].astype(F32)
    first = jnp.concatenate([rows[0:1], rows[1:2, :LANES]], axis=1)
    second = jnp.concatenate([rows[1:2, LANES:], rows[2:3]], axis=1)
    own = jnp.concatenate([first, second], axis=0)
    own_ref[...] = own.astype(BF)
    out_ref[...] = jnp.broadcast_to(own[None], out_ref.shape).astype(BF)


def spread(rows, n):
    piece = (2, rows.size // 2)
    return pl.pallas_call(
        spread_kernel,
        out_shape=(jax.ShapeDtypeStruct((n, *piece), BF), jax.ShapeDtypeStruct(piece, BF)),
        in_specs=[VMEM],
        out_specs=(VMEM, VMEM),
        compiler_params=SMALL,
        cost_estimate=pl.CostEstimate(flops=10**10, bytes_accessed=10**7, transcendentals=0),
        name="spread",
    )(rows)


def step_kernel(b, seqs, kc, vc, parts_ref, shift_ref, fade_ref, state_ref, out_ref, d_ref, k_ref, v_ref):
    total = jnp.sum(parts_ref[...].astype(F32), axis=0)
    tiles = [total[:, k : k + LANES] for k in range(0, total.shape[1], LANES)]
    row = lax.broadcasted_iota(jnp.int32, tiles[0].shape, 0)
    lane = lax.broadcasted_iota(jnp.int32, tiles[0].shape, 1)

    def from_blank(first, second, third):
        second, third = pltpu.roll(second, 4, 0), pltpu.roll(third, 6, 0)
        return jnp.where(row < 2, pltpu.roll(first, 2, 0), jnp.where(row < 4, second, third))

    tiles.append(from_blank(*tiles[:3]))
    squares = jnp.where(lane == row >> 1, from_blank(*tiles[3:4] * 3), 0.0)
    inv_rms = lax.rsqrt(jnp.sum(squares, axis=1, keepdims=True)[:seqs] / D + 1e-06)
    total = jnp.concatenate(tiles, axis=1)[:seqs] * inv_rms
    cols = 3 * kc + 2 * vc
    queries = total[:, :kc] * DK ** (-0.5)
    keys = total[:, kc : 2 * kc]
    pre = total[:, 2 * kc : 3 * kc] + shift_ref[b : b + 1, :]
    values = total[:, 3 * kc : 3 * kc + vc]
    gates = total[:, 3 * kc + vc : cols]
    log_sigmoid = jnp.minimum(pre, 0.0) - jnp.log1p(jnp.exp(-jnp.abs(pre)))
    fade = jnp.concatenate([fade_ref[s : s + 1, b, :] for s in SEQ_OF_ROW], axis=0)
    decay = jnp.exp(log_sigmoid / 16.0 + fade)
    fresh_part = jnp.sum(queries * keys, axis=1, keepdims=True) * values
    columns = jnp.concatenate([queries * decay, jnp.zeros((PAD - seqs, kc), F32)], axis=0).T
    old = [
        jnp.sum(columns[:, j : j + 1] * state_ref[b, s], axis=0, keepdims=True)
        for j, s in enumerate(SEQ_OF_ROW)
    ]
    readout = jnp.concatenate(old, axis=0) + fresh_part
    gated = readout * (gates / (1.0 + jnp.exp(-gates)))
    gated = jnp.concatenate([gated, jnp.zeros((PAD - seqs, vc), F32)], axis=0)
    out_ref[...] = jnp.broadcast_to(gated[None], out_ref.shape).astype(BF)
    for j, s in enumerate(SEQ_OF_ROW):
        d_ref[s : s + 1] = decay[j : j + 1]
        k_ref[s : s + 1] = keys[j : j + 1]
        v_ref[s : s + 1] = values[j : j + 1]


def step(b, parts, shift, fade, state):
    seqs, _, kc = fade.shape
    vc = state.shape[3]
    return pl.pallas_call(
        functools.partial(step_kernel, b, seqs, kc, vc),
        out_shape=(
            jax.ShapeDtypeStruct((parts.shape[0], PAD, vc), BF),
            jax.ShapeDtypeStruct((seqs, kc), F32),
            jax.ShapeDtypeStruct((seqs, kc), F32),
            jax.ShapeDtypeStruct((seqs, vc), F32),
        ),
        in_specs=[VMEM] * 4,
        out_specs=(VMEM,) * 4,
        compiler_params=SMALL,
        name="step",
    )(parts, shift, fade, state)


def readback_kernel(b, gated_ref, weight_ref, out_ref):
    groups, pad, width = gated_ref.shape
    gated = gated_ref[...].astype(F32).reshape(groups * pad, width).astype(BF)
    n = 6 * groups
    i = lax.broadcasted_iota(jnp.int32, (n, groups * pad), 0)
    column = lax.broadcasted_iota(jnp.int32, (n, groups * pad), 1)
    piece = lax.rem(i, 2 * groups)
    group = ((piece >> 1) + groups - shift_between()) & (groups - 1)
    source = group * pad + 2 * lax.div(i, 2 * groups) + (piece & 1)
    chosen = jnp.where(column == source, 1.0, 0.0).astype(BF)
    gated = jnp.dot(chosen, gated, preferred_element_type=F32).astype(BF)
    branch = jnp.dot(gated, weight_ref[b], preferred_element_type=F32)
    one, two, three = (branch[k * 2 * groups : (k + 1) * 2 * groups] for k in range(3))
    first = jnp.concatenate([one, two[:, :LANES]], axis=1)
    second = jnp.concatenate([two[:, LANES:], three], axis=1)
    out_ref[...] = jnp.stack([first, second], axis=1).astype(BF)


def readback(b, gated, weight):
    groups = gated.shape[0]
    return pl.pallas_call(
        functools.partial(readback_kernel, b),
        out_shape=jax.ShapeDtypeStruct((2 * groups, 2, 3 * weight.shape[2] // 2), BF),
        in_specs=[VMEM] * 2,
        out_specs=VMEM,
        compiler_params=SMALL,
        name="readback",
    )(gated, weight)


def shards(
    incoming_embeddings,
    rescale_factors,
    probe_lift,
    address_lift,
    forget_lift,
    forget_shift,
    surplus_fade,
    content_lift,
    filter_lift,
    readback_lift,
    memory_tensor,
):
    weights = (probe_lift, address_lift, forget_lift, content_lift, filter_lift)
    depth = lax.axis_size("z")
    fade = jnp.transpose(surplus_fade, (1, 0, 2))
    copies, stream = spread(incoming_embeddings, 2 * depth)
    kept = []
    for b in range(BLOCKS):
        pieces = exchange(copies, TP)
        parts = exchange(project(b, pieces, rescale_factors, weights), DP)
        gated, *small = step(b, parts, forget_shift, fade, memory_tensor)
        kept.append(small)
        gathered = exchange(gated, DP)
        if b == BLOCKS - 1:
            gathered, kept = lax.optimization_barrier((gathered, kept))
        heads = exchange(readback(b, gathered, readback_lift), TP)
        branch = jnp.sum(heads.astype(F32), axis=0)
        stream = (stream.astype(F32) + branch).astype(BF)
        copies = jnp.broadcast_to(stream[None], copies.shape)
    fresh = [
        memory_tensor[b] * d[:, :, None] + k[:, :, None] * v[:, None, :]
        for b, (d, k, v) in enumerate(kept)
    ]
    return stream.reshape(incoming_embeddings.shape), jnp.stack(fresh)


def solution(mesh):
    z = mesh.shape["tp"] // 2
    fine = Mesh(mesh.devices.reshape(z, 2, 4, 4), ("z", "c", "y", "x"))
    in_specs = (
        P(TP, DP),
        P(None, DP),
        P(None, DP, TP),
        P(None, DP, TP),
        P(None, DP, TP),
        P(None, TP),
        P(None, DP, TP),
        P(None, DP, TP),
        P(None, DP, TP),
        P(None, TP, DP),
        P(None, DP, None, TP),
    )
    out_specs = (P(TP, DP), P(None, DP, None, TP))
    return jax.shard_map(shards, mesh=fine, in_specs=in_specs, out_specs=out_specs, check_vma=False)
```

```python
import functools

import jax
import jax.numpy as jnp
from jax import lax
from jax.experimental import pallas as pl
from jax.experimental.pallas import tpu as pltpu
from jax.sharding import Mesh, PartitionSpec as P

D = 4096
DK = 128
BLOCKS = 2
PAD = 8
LANES = 128
BF = jnp.bfloat16
F32 = jnp.float32
DP = ("y", "x")
TP = ("z", "c")
VMEM = pl.BlockSpec(memory_space=pltpu.VMEM)
SMALL = pltpu.CompilerParams(vmem_limit_bytes=12 * 1024 * 1024)


ORDER = {
    "z": tuple((8 + k) % 16 for k in range(16)),
    DP: tuple((10 + k) % 16 for k in range(16)),
}
ORDER[TP] = tuple(2 * z + c for z in ORDER["z"] for c in (1, 0))
SEQ_OF_ROW = (3, 0, 4, 1, 5, 2)


def exchange(parts, axis):
    return lax.all_to_all(parts, axis, 0, 0, tiled=True, axis_index_groups=[list(ORDER[axis])])


def shift_between():
    return (ORDER[DP][0] - ORDER["z"][0]) % len(ORDER["z"])


def project_kernel(b, pieces_ref, gain_ref, *refs):
    *weights, out_ref = refs
    groups = pieces_ref.shape[0] // 2
    pieces = pieces_ref[...].astype(F32)
    first, second = pieces[:, 0, :], pieces[:, 1, :]
    at = 2 * LANES
    mixed = jnp.concatenate([first[:, at:], second[:, :LANES]], axis=1)
    rows = jnp.concatenate([first[:, :at], mixed, second[:, LANES:]], axis=0).astype(BF)
    i = lax.broadcasted_iota(jnp.int32, (groups * PAD, rows.shape[0]), 0)
    column = lax.broadcasted_iota(jnp.int32, (groups * PAD, rows.shape[0]), 1)
    piece = 2 * (((i >> 3) + shift_between()) & (groups - 1)) + (i & 1)
    chosen = jnp.where(column == ((i & 7) >> 1) * 2 * groups + piece, 1.0, 0.0).astype(BF)
    rows = jnp.dot(chosen, rows, preferred_element_type=F32)
    squares = jnp.sum(rows * rows, axis=1, keepdims=True)
    hidden = (rows * gain_ref[b : b + 1, :].astype(F32)).astype(BF)
    tiles = []
    for w in weights:
        part = jnp.dot(hidden, w[b], preferred_element_type=F32)
        tiles += [part[:, k : k + LANES] for k in range(0, part.shape[1], LANES)]
    last = tiles.pop()
    row = lax.broadcasted_iota(jnp.int32, last.shape, 0) & 7
    lane = lax.broadcasted_iota(jnp.int32, last.shape, 1)
    spread_squares = jnp.broadcast_to(squares, last.shape)
    moved = [pltpu.roll(spread_squares, k, 0) for k in (6, 4, 2)]
    extra = [pltpu.roll(last, k, 0) for k in (6, 4, 2)]
    extra.append(jnp.where(lane == 0, moved[0], jnp.where(lane == 1, moved[1], moved[2])))
    for k, tile in enumerate(tiles):
        if k < len(extra):
            tile = jnp.where(row >= 6, extra[k], tile)
        out_ref[:, :, k * LANES : (k + 1) * LANES] = tile.reshape(groups, PAD, LANES).astype(BF)


def project(b, pieces, gain, weights):
    cols = sum(w.shape[2] for w in weights) - LANES
    return pl.pallas_call(
        functools.partial(project_kernel, b),
        out_shape=jax.ShapeDtypeStruct((pieces.shape[0] // 2, PAD, cols), BF),
        in_specs=[VMEM] * (2 + len(weights)),
        out_specs=VMEM,
        compiler_params=SMALL,
        name="project",
    )(pieces, gain, *weights)


def spread_kernel(rows_ref, out_ref, own_ref):
    rows = rows_ref[...].astype(F32)
    first = jnp.concatenate([rows[0:1], rows[1:2, :LANES]], axis=1)
    second = jnp.concatenate([rows[1:2, LANES:], rows[2:3]], axis=1)
    own = jnp.concatenate([first, second], axis=0)
    own_ref[...] = own.astype(BF)
    out_ref[...] = jnp.broadcast_to(own[None], out_ref.shape).astype(BF)


def spread(rows, n):
    piece = (2, rows.size // 2)
    return pl.pallas_call(
        spread_kernel,
        out_shape=(jax.ShapeDtypeStruct((n, *piece), BF), jax.ShapeDtypeStruct(piece, BF)),
        in_specs=[VMEM],
        out_specs=(VMEM, VMEM),
        compiler_params=SMALL,
        name="spread",
    )(rows)


def hold_kernel(in_ref, out_ref):
    out_ref[0] = in_ref[0]


def hold(copies):
    return pl.pallas_call(
        hold_kernel,
        out_shape=jax.ShapeDtypeStruct(copies.shape, copies.dtype),
        in_specs=[VMEM],
        out_specs=VMEM,
        input_output_aliases={0: 0},
        compiler_params=SMALL,
        cost_estimate=pl.CostEstimate(flops=10**10, bytes_accessed=10**7, transcendentals=0),
        name="hold",
    )(copies)


def finish_kernel(heads_ref, stream_ref, out_ref):
    total = jnp.sum(heads_ref[...].astype(F32), axis=0) + stream_ref[...].astype(F32)
    first, second = total[0:1], total[1:2]
    at = 2 * LANES
    middle = jnp.concatenate([first[:, at:], second[:, :LANES]], axis=1)
    out_ref[...] = jnp.concatenate([first[:, :at], middle, second[:, LANES:]], axis=0).astype(BF)


def finish(heads, stream, shape):
    return pl.pallas_call(
        finish_kernel,
        out_shape=jax.ShapeDtypeStruct(shape, BF),
        in_specs=[VMEM] * 2,
        out_specs=VMEM,
        compiler_params=SMALL,
        name="finish",
    )(heads, stream)


def step_kernel(b, seqs, kc, vc, parts_ref, shift_ref, fade_ref, state_ref, out_ref, d_ref, k_ref, v_ref):
    total = jnp.sum(parts_ref[...].astype(F32), axis=0)
    tiles = [total[:, k : k + LANES] for k in range(0, total.shape[1], LANES)]
    row = lax.broadcasted_iota(jnp.int32, tiles[0].shape, 0)
    lane = lax.broadcasted_iota(jnp.int32, tiles[0].shape, 1)

    def from_blank(first, second, third):
        second, third = pltpu.roll(second, 4, 0), pltpu.roll(third, 6, 0)
        return jnp.where(row < 2, pltpu.roll(first, 2, 0), jnp.where(row < 4, second, third))

    tiles.append(from_blank(*tiles[:3]))
    squares = jnp.where(lane == row >> 1, from_blank(*tiles[3:4] * 3), 0.0)
    inv_rms = lax.rsqrt(jnp.sum(squares, axis=1, keepdims=True)[:seqs] / D + 1e-06)
    total = jnp.concatenate(tiles, axis=1)[:seqs] * inv_rms
    cols = 3 * kc + 2 * vc
    queries = total[:, :kc] * DK ** (-0.5)
    keys = total[:, kc : 2 * kc]
    pre = total[:, 2 * kc : 3 * kc] + shift_ref[b : b + 1, :]
    values = total[:, 3 * kc : 3 * kc + vc]
    gates = total[:, 3 * kc + vc : cols]
    log_sigmoid = jnp.minimum(pre, 0.0) - jnp.log1p(jnp.exp(-jnp.abs(pre)))
    fade = jnp.concatenate([fade_ref[s : s + 1, b, :] for s in SEQ_OF_ROW], axis=0)
    decay = jnp.exp(log_sigmoid / 16.0 + fade)
    fresh_part = jnp.sum(queries * keys, axis=1, keepdims=True) * values
    columns = jnp.concatenate([queries * decay, jnp.zeros((PAD - seqs, kc), F32)], axis=0).T
    old = [
        jnp.sum(columns[:, j : j + 1] * state_ref[b, s], axis=0, keepdims=True)
        for j, s in enumerate(SEQ_OF_ROW)
    ]
    readout = jnp.concatenate(old, axis=0) + fresh_part
    gated = readout * (gates / (1.0 + jnp.exp(-gates)))
    gated = jnp.concatenate([gated, jnp.zeros((PAD - seqs, vc), F32)], axis=0)
    out_ref[...] = jnp.broadcast_to(gated[None], out_ref.shape).astype(BF)
    for j, s in enumerate(SEQ_OF_ROW):
        d_ref[s : s + 1] = decay[j : j + 1]
        k_ref[s : s + 1] = keys[j : j + 1]
        v_ref[s : s + 1] = values[j : j + 1]


def step(b, parts, shift, fade, state):
    seqs, _, kc = fade.shape
    vc = state.shape[3]
    return pl.pallas_call(
        functools.partial(step_kernel, b, seqs, kc, vc),
        out_shape=(
            jax.ShapeDtypeStruct((parts.shape[0], PAD, vc), BF),
            jax.ShapeDtypeStruct((seqs, kc), F32),
            jax.ShapeDtypeStruct((seqs, kc), F32),
            jax.ShapeDtypeStruct((seqs, vc), F32),
        ),
        in_specs=[VMEM] * 4,
        out_specs=(VMEM,) * 4,
        compiler_params=SMALL,
        name="step",
    )(parts, shift, fade, state)


def readback_kernel(b, gated_ref, weight_ref, out_ref):
    groups, pad, width = gated_ref.shape
    gated = gated_ref[...].astype(F32).reshape(groups * pad, width).astype(BF)
    n = 6 * groups
    i = lax.broadcasted_iota(jnp.int32, (n, groups * pad), 0)
    column = lax.broadcasted_iota(jnp.int32, (n, groups * pad), 1)
    piece = lax.rem(i, 2 * groups)
    group = ((piece >> 1) + groups - shift_between()) & (groups - 1)
    source = group * pad + 2 * lax.div(i, 2 * groups) + (piece & 1)
    chosen = jnp.where(column == source, 1.0, 0.0).astype(BF)
    gated = jnp.dot(chosen, gated, preferred_element_type=F32).astype(BF)
    branch = jnp.dot(gated, weight_ref[b], preferred_element_type=F32)
    one, two, three = (branch[k * 2 * groups : (k + 1) * 2 * groups] for k in range(3))
    first = jnp.concatenate([one, two[:, :LANES]], axis=1)
    second = jnp.concatenate([two[:, LANES:], three], axis=1)
    out_ref[...] = jnp.stack([first, second], axis=1).astype(BF)


def readback(b, gated, weight):
    groups = gated.shape[0]
    return pl.pallas_call(
        functools.partial(readback_kernel, b),
        out_shape=jax.ShapeDtypeStruct((2 * groups, 2, 3 * weight.shape[2] // 2), BF),
        in_specs=[VMEM] * 2,
        out_specs=VMEM,
        compiler_params=SMALL,
        name="readback",
    )(gated, weight)


def shards(
    incoming_embeddings,
    rescale_factors,
    probe_lift,
    address_lift,
    forget_lift,
    forget_shift,
    surplus_fade,
    content_lift,
    filter_lift,
    readback_lift,
    memory_tensor,
):
    weights = (probe_lift, address_lift, forget_lift, content_lift, filter_lift)
    depth = lax.axis_size("z")
    fade = jnp.transpose(surplus_fade, (1, 0, 2))
    copies, stream = spread(incoming_embeddings, 2 * depth)
    copies = hold(copies)
    kept = []
    for b in range(BLOCKS):
        pieces = exchange(copies, TP)
        parts = exchange(project(b, pieces, rescale_factors, weights), DP)
        gated, *small = step(b, parts, forget_shift, fade, memory_tensor)
        kept.append(small)
        gathered = exchange(gated, DP)
        if b == BLOCKS - 1:
            gathered, kept = lax.optimization_barrier((gathered, kept))
        heads = exchange(readback(b, gathered, readback_lift), TP)
        if b == BLOCKS - 1:
            mixed = finish(heads, stream, incoming_embeddings.shape)
            break
        branch = jnp.sum(heads.astype(F32), axis=0)
        stream = (stream.astype(F32) + branch).astype(BF)
        copies = jnp.broadcast_to(stream[None], copies.shape)
    fresh = [
        memory_tensor[b] * d[:, :, None] + k[:, :, None] * v[:, None, :]
        for b, (d, k, v) in enumerate(kept)
    ]
    return mixed, jnp.stack(fresh)


def solution(mesh):
    z = mesh.shape["tp"] // 2
    fine = Mesh(mesh.devices.reshape(z, 2, 4, 4), ("z", "c", "y", "x"))
    in_specs = (
        P(TP, DP),
        P(None, DP),
        P(None, DP, TP),
        P(None, DP, TP),
        P(None, DP, TP),
        P(None, TP),
        P(None, DP, TP),
        P(None, DP, TP),
        P(None, DP, TP),
        P(None, TP, DP),
        P(None, DP, None, TP),
    )
    out_specs = (P(TP, DP), P(None, DP, None, TP))
    return jax.shard_map(shards, mesh=fine, in_specs=in_specs, out_specs=out_specs, check_vma=False)
```

```python
import functools

import jax
import jax.numpy as jnp
from jax import lax
from jax.experimental import pallas as pl
from jax.experimental.pallas import tpu as pltpu
from jax.sharding import Mesh, PartitionSpec as P

D = 4096
DK = 128
BLOCKS = 2
PAD = 8
LANES = 128
BF = jnp.bfloat16
F32 = jnp.float32
DP = ("y", "x")
TP = ("z", "c")
VMEM = pl.BlockSpec(memory_space=pltpu.VMEM)
SMALL = pltpu.CompilerParams(vmem_limit_bytes=12 * 1024 * 1024)


ORDER = {
    "z": tuple((8 + k) % 16 for k in range(16)),
    DP: tuple((10 + k) % 16 for k in range(16)),
}
ORDER[TP] = tuple(2 * z + c for z in ORDER["z"] for c in (1, 0))
SEQ_OF_ROW = (3, 0, 4, 1, 5, 2)


def exchange(parts, axis):
    return lax.all_to_all(parts, axis, 0, 0, tiled=True, axis_index_groups=[list(ORDER[axis])])


def shift_between():
    return (ORDER[DP][0] - ORDER["z"][0]) % len(ORDER["z"])


def project_kernel(b, pieces_ref, gain_ref, *refs):
    *weights, out_ref = refs
    groups = pieces_ref.shape[0] // 2
    pieces = pieces_ref[...].astype(F32)
    first, second = pieces[:, 0, :], pieces[:, 1, :]
    at = 2 * LANES
    mixed = jnp.concatenate([first[:, at:], second[:, :LANES]], axis=1)
    rows = jnp.concatenate([first[:, :at], mixed, second[:, LANES:]], axis=0).astype(BF)
    i = lax.broadcasted_iota(jnp.int32, (groups * PAD, rows.shape[0]), 0)
    column = lax.broadcasted_iota(jnp.int32, (groups * PAD, rows.shape[0]), 1)
    piece = 2 * (((i >> 3) + shift_between()) & (groups - 1)) + (i & 1)
    chosen = jnp.where(column == ((i & 7) >> 1) * 2 * groups + piece, 1.0, 0.0).astype(BF)
    rows = jnp.dot(chosen, rows, preferred_element_type=F32)
    squares = jnp.sum(rows * rows, axis=1, keepdims=True)
    hidden = (rows * gain_ref[b : b + 1, :].astype(F32)).astype(BF)
    tiles = []
    for w in weights:
        part = jnp.dot(hidden, w[b], preferred_element_type=F32)
        tiles += [part[:, k : k + LANES] for k in range(0, part.shape[1], LANES)]
    last = tiles.pop()
    row = lax.broadcasted_iota(jnp.int32, last.shape, 0) & 7
    lane = lax.broadcasted_iota(jnp.int32, last.shape, 1)
    spread_squares = jnp.broadcast_to(squares, last.shape)
    moved = [pltpu.roll(spread_squares, k, 0) for k in (6, 4, 2)]
    extra = [pltpu.roll(last, k, 0) for k in (6, 4, 2)]
    extra.append(jnp.where(lane == 0, moved[0], jnp.where(lane == 1, moved[1], moved[2])))
    for k, tile in enumerate(tiles):
        if k < len(extra):
            tile = jnp.where(row >= 6, extra[k], tile)
        out_ref[:, :, k * LANES : (k + 1) * LANES] = tile.reshape(groups, PAD, LANES).astype(BF)


def project(b, pieces, gain, weights):
    cols = sum(w.shape[2] for w in weights) - LANES
    return pl.pallas_call(
        functools.partial(project_kernel, b),
        out_shape=jax.ShapeDtypeStruct((pieces.shape[0] // 2, PAD, cols), BF),
        in_specs=[VMEM] * (2 + len(weights)),
        out_specs=VMEM,
        compiler_params=SMALL,
        name="project",
    )(pieces, gain, *weights)


def spread_kernel(rows_ref, out_ref, own_ref):
    rows = rows_ref[...].astype(F32)
    first = jnp.concatenate([rows[0:1], rows[1:2, :LANES]], axis=1)
    second = jnp.concatenate([rows[1:2, LANES:], rows[2:3]], axis=1)
    own = jnp.concatenate([first, second], axis=0)
    own_ref[...] = own.astype(BF)
    out_ref[...] = jnp.broadcast_to(own[None], out_ref.shape).astype(BF)


def spread(rows, n):
    piece = (2, rows.size // 2)
    return pl.pallas_call(
        spread_kernel,
        out_shape=(jax.ShapeDtypeStruct((n, *piece), BF), jax.ShapeDtypeStruct(piece, BF)),
        in_specs=[VMEM],
        out_specs=(VMEM, VMEM),
        compiler_params=SMALL,
        name="spread",
    )(rows)


def hold_kernel(in_ref, out_ref):
    out_ref[0] = in_ref[0]


def hold(copies):
    return pl.pallas_call(
        hold_kernel,
        out_shape=jax.ShapeDtypeStruct(copies.shape, copies.dtype),
        in_specs=[VMEM],
        out_specs=VMEM,
        input_output_aliases={0: 0},
        compiler_params=SMALL,
        cost_estimate=pl.CostEstimate(flops=10**10, bytes_accessed=10**7, transcendentals=0),
        name="hold",
    )(copies)


def finish_kernel(heads_ref, stream_ref, out_ref):
    total = jnp.sum(heads_ref[...].astype(F32), axis=0) + stream_ref[...].astype(F32)
    first, second = total[0:1], total[1:2]
    at = 2 * LANES
    middle = jnp.concatenate([first[:, at:], second[:, :LANES]], axis=1)
    out_ref[...] = jnp.concatenate([first[:, :at], middle, second[:, LANES:]], axis=0).astype(BF)


def finish(heads, stream, shape):
    return pl.pallas_call(
        finish_kernel,
        out_shape=jax.ShapeDtypeStruct(shape, BF),
        in_specs=[VMEM] * 2,
        out_specs=VMEM,
        compiler_params=SMALL,
        name="finish",
    )(heads, stream)


def step_kernel(b, seqs, kc, vc, parts_ref, shift_ref, fade_ref, state_ref, out_ref, d_ref, k_ref, v_ref):
    total = jnp.sum(parts_ref[...].astype(F32), axis=0)
    tiles = [total[:, k : k + LANES] for k in range(0, total.shape[1], LANES)]
    row = lax.broadcasted_iota(jnp.int32, tiles[0].shape, 0)
    lane = lax.broadcasted_iota(jnp.int32, tiles[0].shape, 1)

    def from_blank(first, second, third):
        second, third = pltpu.roll(second, 4, 0), pltpu.roll(third, 6, 0)
        return jnp.where(row < 2, pltpu.roll(first, 2, 0), jnp.where(row < 4, second, third))

    tiles.append(from_blank(*tiles[:3]))
    squares = jnp.where(lane == row >> 1, from_blank(*tiles[3:4] * 3), 0.0)
    inv_rms = lax.rsqrt(jnp.sum(squares, axis=1, keepdims=True)[:seqs] / D + 1e-06)
    total = jnp.concatenate(tiles, axis=1)[:seqs] * inv_rms
    cols = 3 * kc + 2 * vc
    queries = total[:, :kc] * DK ** (-0.5)
    keys = total[:, kc : 2 * kc]
    pre = total[:, 2 * kc : 3 * kc] + shift_ref[b : b + 1, :]
    values = total[:, 3 * kc : 3 * kc + vc]
    gates = total[:, 3 * kc + vc : cols]
    log_sigmoid = jnp.minimum(pre, 0.0) - jnp.log1p(jnp.exp(-jnp.abs(pre)))
    fade = jnp.concatenate([fade_ref[s : s + 1, b, :] for s in SEQ_OF_ROW], axis=0)
    decay = jnp.exp(log_sigmoid / 16.0 + fade)
    fresh_part = jnp.sum(queries * keys, axis=1, keepdims=True) * values
    columns = jnp.concatenate([queries * decay, jnp.zeros((PAD - seqs, kc), F32)], axis=0).T
    old = [
        jnp.sum(columns[:, j : j + 1] * state_ref[b, s], axis=0, keepdims=True)
        for j, s in enumerate(SEQ_OF_ROW)
    ]
    readout = jnp.concatenate(old, axis=0) + fresh_part
    gated = readout * (gates / (1.0 + jnp.exp(-gates)))
    chunks = [gated[j : j + 1, k : k + LANES] for j in range(seqs) for k in range(0, vc, LANES)]
    packed = [jnp.concatenate(chunks[k : k + 3], axis=1) for k in range(0, len(chunks), 3)]
    out_ref[...] = jnp.broadcast_to(jnp.concatenate(packed, axis=0)[None], out_ref.shape).astype(BF)
    for j, s in enumerate(SEQ_OF_ROW):
        d_ref[s : s + 1] = decay[j : j + 1]
        k_ref[s : s + 1] = keys[j : j + 1]
        v_ref[s : s + 1] = values[j : j + 1]


def step(b, parts, shift, fade, state):
    seqs, _, kc = fade.shape
    vc = state.shape[3]
    return pl.pallas_call(
        functools.partial(step_kernel, b, seqs, kc, vc),
        out_shape=(
            jax.ShapeDtypeStruct((parts.shape[0], seqs * vc // (3 * LANES), 3 * LANES), BF),
            jax.ShapeDtypeStruct((seqs, kc), F32),
            jax.ShapeDtypeStruct((seqs, kc), F32),
            jax.ShapeDtypeStruct((seqs, vc), F32),
        ),
        in_specs=[VMEM] * 4,
        out_specs=(VMEM,) * 4,
        compiler_params=SMALL,
        name="step",
    )(parts, shift, fade, state)


def readback_kernel(b, gated_ref, weight_ref, out_ref):
    groups, packed, width = gated_ref.shape
    flat = gated_ref[...].astype(F32).reshape(groups * packed, width).astype(BF)
    chunks = jnp.concatenate([flat[:, k : k + LANES] for k in range(0, width, LANES)], axis=0)
    i = lax.broadcasted_iota(jnp.int32, (6 * groups, chunks.shape[0]), 0)
    column = lax.broadcasted_iota(jnp.int32, (6 * groups, chunks.shape[0]), 1)
    piece = lax.rem(i, 2 * groups)
    group = ((piece >> 1) + groups - shift_between()) & (groups - 1)
    halves = []
    for half in (0, 1):
        chunk = 4 * lax.div(i, 2 * groups) + 2 * (piece & 1) + half
        row = (chunk * 11) >> 5
        source = ((chunk - 3 * row) * groups + group) * packed + row
        chosen = jnp.where(column == source, 1.0, 0.0).astype(BF)
        halves.append(jnp.dot(chosen, chunks, preferred_element_type=F32))
    gated = jnp.concatenate(halves, axis=1).astype(BF)
    branch = jnp.dot(gated, weight_ref[b], preferred_element_type=F32)
    one, two, three = (branch[k * 2 * groups : (k + 1) * 2 * groups] for k in range(3))
    first = jnp.concatenate([one, two[:, :LANES]], axis=1)
    second = jnp.concatenate([two[:, LANES:], three], axis=1)
    out_ref[...] = jnp.stack([first, second], axis=1).astype(BF)


def readback(b, gated, weight):
    groups = gated.shape[0]
    return pl.pallas_call(
        functools.partial(readback_kernel, b),
        out_shape=jax.ShapeDtypeStruct((2 * groups, 2, 3 * weight.shape[2] // 2), BF),
        in_specs=[VMEM] * 2,
        out_specs=VMEM,
        compiler_params=SMALL,
        name="readback",
    )(gated, weight)


def shards(
    incoming_embeddings,
    rescale_factors,
    probe_lift,
    address_lift,
    forget_lift,
    forget_shift,
    surplus_fade,
    content_lift,
    filter_lift,
    readback_lift,
    memory_tensor,
):
    weights = (probe_lift, address_lift, forget_lift, content_lift, filter_lift)
    depth = lax.axis_size("z")
    fade = jnp.transpose(surplus_fade, (1, 0, 2))
    copies, stream = spread(incoming_embeddings, 2 * depth)
    copies = hold(copies)
    kept = []
    for b in range(BLOCKS):
        pieces = exchange(copies, TP)
        parts = exchange(project(b, pieces, rescale_factors, weights), DP)
        gated, *small = step(b, parts, forget_shift, fade, memory_tensor)
        kept.append(small)
        gathered = exchange(gated, DP)
        if b == BLOCKS - 1:
            gathered, kept = lax.optimization_barrier((gathered, kept))
        heads = exchange(readback(b, gathered, readback_lift), TP)
        if b == BLOCKS - 1:
            mixed = finish(heads, stream, incoming_embeddings.shape)
            break
        branch = jnp.sum(heads.astype(F32), axis=0)
        stream = (stream.astype(F32) + branch).astype(BF)
        copies = jnp.broadcast_to(stream[None], copies.shape)
    fresh = [
        memory_tensor[b] * d[:, :, None] + k[:, :, None] * v[:, None, :]
        for b, (d, k, v) in enumerate(kept)
    ]
    return mixed, jnp.stack(fresh)


def solution(mesh):
    z = mesh.shape["tp"] // 2
    fine = Mesh(mesh.devices.reshape(z, 2, 4, 4), ("z", "c", "y", "x"))
    in_specs = (
        P(TP, DP),
        P(None, DP),
        P(None, DP, TP),
        P(None, DP, TP),
        P(None, DP, TP),
        P(None, TP),
        P(None, DP, TP),
        P(None, DP, TP),
        P(None, DP, TP),
        P(None, TP, DP),
        P(None, DP, None, TP),
    )
    out_specs = (P(TP, DP), P(None, DP, None, TP))
    return jax.shard_map(shards, mesh=fine, in_specs=in_specs, out_specs=out_specs, check_vma=False)
```

```python
import functools

import jax
import jax.numpy as jnp
from jax import lax
from jax.experimental import pallas as pl
from jax.experimental.pallas import tpu as pltpu
from jax.sharding import Mesh, PartitionSpec as P

D = 4096
DK = 128
BLOCKS = 2
PAD = 8
LANES = 128
BF = jnp.bfloat16
F32 = jnp.float32
DP = ("y", "x")
TP = ("z", "c")
VMEM = pl.BlockSpec(memory_space=pltpu.VMEM)
SMALL = pltpu.CompilerParams(vmem_limit_bytes=12 * 1024 * 1024)


ORDER = {
    "z": tuple((8 + k) % 16 for k in range(16)),
    DP: tuple((10 + k) % 16 for k in range(16)),
}
ORDER[TP] = tuple(2 * z + c for z in ORDER["z"] for c in (1, 0))
SEQ_OF_ROW = (3, 0, 4, 1, 5, 2)


def exchange(parts, axis):
    return lax.all_to_all(parts, axis, 0, 0, tiled=True, axis_index_groups=[list(ORDER[axis])])


def shift_between():
    return (ORDER[DP][0] - ORDER["z"][0]) % len(ORDER["z"])


def project_kernel(b, pieces_ref, gain_ref, *refs):
    *weights, out_ref = refs
    groups = pieces_ref.shape[0] // 2
    pieces = pieces_ref[...].astype(F32)
    first, second = pieces[:, 0, :], pieces[:, 1, :]
    at = 2 * LANES
    mixed = jnp.concatenate([first[:, at:], second[:, :LANES]], axis=1)
    rows = jnp.concatenate([first[:, :at], mixed, second[:, LANES:]], axis=0).astype(BF)
    i = lax.broadcasted_iota(jnp.int32, (groups * PAD, rows.shape[0]), 0)
    column = lax.broadcasted_iota(jnp.int32, (groups * PAD, rows.shape[0]), 1)
    piece = 2 * (((i >> 3) + shift_between()) & (groups - 1)) + (i & 1)
    chosen = jnp.where(column == ((i & 7) >> 1) * 2 * groups + piece, 1.0, 0.0).astype(BF)
    rows = jnp.dot(chosen, rows, preferred_element_type=F32)
    squares = jnp.sum(rows * rows, axis=1, keepdims=True)
    hidden = (rows * gain_ref[b : b + 1, :].astype(F32)).astype(BF)
    tiles = []
    for w in weights:
        part = jnp.dot(hidden, w[b], preferred_element_type=F32)
        tiles += [part[:, k : k + LANES] for k in range(0, part.shape[1], LANES)]
    last = tiles.pop()
    row = lax.broadcasted_iota(jnp.int32, last.shape, 0) & 7
    lane = lax.broadcasted_iota(jnp.int32, last.shape, 1)
    spread_squares = jnp.broadcast_to(squares, last.shape)
    moved = [pltpu.roll(spread_squares, k, 0) for k in (6, 4, 2)]
    extra = [pltpu.roll(last, k, 0) for k in (6, 4, 2)]
    extra.append(jnp.where(lane == 0, moved[0], jnp.where(lane == 1, moved[1], moved[2])))
    for k, tile in enumerate(tiles):
        if k < len(extra):
            tile = jnp.where(row >= 6, extra[k], tile)
        out_ref[:, :, k * LANES : (k + 1) * LANES] = tile.reshape(groups, PAD, LANES).astype(BF)


def project(b, pieces, gain, weights):
    cols = sum(w.shape[2] for w in weights) - LANES
    return pl.pallas_call(
        functools.partial(project_kernel, b),
        out_shape=jax.ShapeDtypeStruct((pieces.shape[0] // 2, PAD, cols), BF),
        in_specs=[VMEM] * (2 + len(weights)),
        out_specs=VMEM,
        compiler_params=SMALL,
        name="project",
    )(pieces, gain, *weights)


def spread_kernel(rows_ref, out_ref, own_ref):
    rows = rows_ref[...].astype(F32)
    first = jnp.concatenate([rows[0:1], rows[1:2, :LANES]], axis=1)
    second = jnp.concatenate([rows[1:2, LANES:], rows[2:3]], axis=1)
    own = jnp.concatenate([first, second], axis=0)
    own_ref[...] = own.astype(BF)
    out_ref[...] = jnp.broadcast_to(own[None], out_ref.shape).astype(BF)


def spread(rows, n):
    piece = (2, rows.size // 2)
    return pl.pallas_call(
        spread_kernel,
        out_shape=(jax.ShapeDtypeStruct((n, *piece), BF), jax.ShapeDtypeStruct(piece, BF)),
        in_specs=[VMEM],
        out_specs=(VMEM, VMEM),
        compiler_params=SMALL,
        name="spread",
    )(rows)


def hold_kernel(in_ref, out_ref):
    out_ref[0] = in_ref[0]


def hold(copies):
    return pl.pallas_call(
        hold_kernel,
        out_shape=jax.ShapeDtypeStruct(copies.shape, copies.dtype),
        in_specs=[VMEM],
        out_specs=VMEM,
        input_output_aliases={0: 0},
        compiler_params=SMALL,
        cost_estimate=pl.CostEstimate(flops=10**10, bytes_accessed=10**7, transcendentals=0),
        name="hold",
    )(copies)


def finish_kernel(heads_ref, stream_ref, out_ref):
    total = jnp.sum(heads_ref[...].astype(F32), axis=0) + stream_ref[...].astype(F32)
    first, second = total[0:1], total[1:2]
    at = 2 * LANES
    middle = jnp.concatenate([first[:, at:], second[:, :LANES]], axis=1)
    out_ref[...] = jnp.concatenate([first[:, :at], middle, second[:, LANES:]], axis=0).astype(BF)


def finish(heads, stream, shape):
    return pl.pallas_call(
        finish_kernel,
        out_shape=jax.ShapeDtypeStruct(shape, BF),
        in_specs=[VMEM] * 2,
        out_specs=VMEM,
        compiler_params=SMALL,
        name="finish",
    )(heads, stream)


def step_kernel(b, seqs, kc, vc, parts_ref, shift_ref, fade_ref, state_ref, out_ref, d_ref, k_ref, v_ref):
    total = jnp.sum(parts_ref[...].astype(F32), axis=0)
    tiles = [total[:, k : k + LANES] for k in range(0, total.shape[1], LANES)]
    row = lax.broadcasted_iota(jnp.int32, tiles[0].shape, 0)
    lane = lax.broadcasted_iota(jnp.int32, tiles[0].shape, 1)

    def from_blank(first, second, third):
        second, third = pltpu.roll(second, 4, 0), pltpu.roll(third, 6, 0)
        return jnp.where(row < 2, pltpu.roll(first, 2, 0), jnp.where(row < 4, second, third))

    tiles.append(from_blank(*tiles[:3]))
    squares = jnp.where(lane == row >> 1, from_blank(*tiles[3:4] * 3), 0.0)
    inv_rms = lax.rsqrt(jnp.sum(squares, axis=1, keepdims=True)[:seqs] / D + 1e-06)
    total = jnp.concatenate(tiles, axis=1)[:seqs] * inv_rms
    cols = 3 * kc + 2 * vc
    queries = total[:, :kc] * DK ** (-0.5)
    keys = total[:, kc : 2 * kc]
    pre = total[:, 2 * kc : 3 * kc] + shift_ref[b : b + 1, :]
    values = total[:, 3 * kc : 3 * kc + vc]
    gates = total[:, 3 * kc + vc : cols]
    log_sigmoid = jnp.minimum(pre, 0.0) - jnp.log1p(jnp.exp(-jnp.abs(pre)))
    fade = jnp.concatenate([fade_ref[s : s + 1, b, :] for s in SEQ_OF_ROW], axis=0)
    decay = jnp.exp(log_sigmoid / 16.0 + fade)
    fresh_part = jnp.sum(queries * keys, axis=1, keepdims=True) * values
    columns = jnp.concatenate([queries * decay, jnp.zeros((PAD - seqs, kc), F32)], axis=0).T
    old = [
        jnp.sum(columns[:, j : j + 1] * state_ref[b, s], axis=0, keepdims=True)
        for j, s in enumerate(SEQ_OF_ROW)
    ]
    readout = jnp.concatenate(old, axis=0) + fresh_part
    gated = readout * (gates / (1.0 + jnp.exp(-gates)))
    chunks = [gated[j : j + 1, k : k + LANES] for j in range(seqs) for k in range(0, vc, LANES)]
    packed = [jnp.concatenate(chunks[k : k + 3], axis=1) for k in range(0, len(chunks), 3)]
    out_ref[...] = jnp.broadcast_to(jnp.concatenate(packed, axis=0)[None], out_ref.shape).astype(BF)
    for j, s in enumerate(SEQ_OF_ROW):
        d_ref[s : s + 1] = decay[j : j + 1]
        k_ref[s : s + 1] = keys[j : j + 1]
        v_ref[s : s + 1] = values[j : j + 1]


def step(b, parts, shift, fade, state):
    seqs, _, kc = fade.shape
    vc = state.shape[3]
    return pl.pallas_call(
        functools.partial(step_kernel, b, seqs, kc, vc),
        out_shape=(
            jax.ShapeDtypeStruct((parts.shape[0], seqs * vc // (3 * LANES), 3 * LANES), BF),
            jax.ShapeDtypeStruct((seqs, kc), F32),
            jax.ShapeDtypeStruct((seqs, kc), F32),
            jax.ShapeDtypeStruct((seqs, vc), F32),
        ),
        in_specs=[VMEM] * 4,
        out_specs=(VMEM,) * 4,
        compiler_params=SMALL,
        name="step",
    )(parts, shift, fade, state)


def readback_kernel(b, gated_ref, weight_ref, out_ref):
    groups, packed, width = gated_ref.shape
    flat = gated_ref[...].astype(F32).reshape(groups * packed, width).astype(BF)
    chunks = jnp.concatenate([flat[:, k : k + LANES] for k in range(0, width, LANES)], axis=0)
    i = lax.broadcasted_iota(jnp.int32, (6 * groups, chunks.shape[0]), 0)
    column = lax.broadcasted_iota(jnp.int32, (6 * groups, chunks.shape[0]), 1)
    piece = lax.rem(i, 2 * groups)
    group = ((piece >> 1) + groups - shift_between()) & (groups - 1)
    halves = []
    for half in (0, 1):
        chunk = 4 * lax.div(i, 2 * groups) + 2 * (piece & 1) + half
        row = (chunk * 11) >> 5
        source = ((chunk - 3 * row) * groups + group) * packed + row
        chosen = jnp.where(column == source, 1.0, 0.0).astype(BF)
        halves.append(jnp.dot(chosen, chunks, preferred_element_type=F32))
    gated = jnp.concatenate(halves, axis=1).astype(BF)
    branch = jnp.dot(gated, weight_ref[b], preferred_element_type=F32)
    one, two, three = (branch[k * 2 * groups : (k + 1) * 2 * groups] for k in range(3))
    first = jnp.concatenate([one, two[:, :LANES]], axis=1)
    second = jnp.concatenate([two[:, LANES:], three], axis=1)
    out_ref[...] = jnp.stack([first, second], axis=1).astype(BF)


def readback(b, gated, weight):
    groups = gated.shape[0]
    return pl.pallas_call(
        functools.partial(readback_kernel, b),
        out_shape=jax.ShapeDtypeStruct((2 * groups, 2, 3 * weight.shape[2] // 2), BF),
        in_specs=[VMEM] * 2,
        out_specs=VMEM,
        compiler_params=SMALL,
        name="readback",
    )(gated, weight)


def shards(
    incoming_embeddings,
    rescale_factors,
    probe_lift,
    address_lift,
    forget_lift,
    forget_shift,
    surplus_fade,
    content_lift,
    filter_lift,
    readback_lift,
    memory_tensor,
):
    weights = (probe_lift, address_lift, forget_lift, content_lift, filter_lift)
    depth = lax.axis_size("z")
    fade = jnp.transpose(surplus_fade, (1, 0, 2))
    copies, stream = spread(incoming_embeddings, 2 * depth)
    copies = hold(copies)
    kept = []
    for b in range(BLOCKS):
        pieces = exchange(copies, TP)
        parts = exchange(project(b, pieces, rescale_factors, weights), DP)
        gated, *small = step(b, parts, forget_shift, fade, memory_tensor)
        kept.append(small)
        gathered = exchange(gated, DP)
        if b == BLOCKS - 1:
            gathered, kept = lax.optimization_barrier((gathered, kept))
        heads = exchange(readback(b, gathered, readback_lift), TP)
        if b == BLOCKS - 1:
            mixed = finish(heads, stream, incoming_embeddings.shape)
            break
        branch = jnp.sum(heads.astype(F32), axis=0)
        stream = (stream.astype(F32) + branch).astype(BF)
        copies = jnp.broadcast_to(stream[None], copies.shape)
    decays, keys, values = (jnp.stack(both) for both in zip(*kept))
    fresh = memory_tensor * decays[..., None] + keys[..., None] * values[:, :, None, :]
    return mixed, fresh


def solution(mesh):
    z = mesh.shape["tp"] // 2
    fine = Mesh(mesh.devices.reshape(z, 2, 4, 4), ("z", "c", "y", "x"))
    in_specs = (
        P(TP, DP),
        P(None, DP),
        P(None, DP, TP),
        P(None, DP, TP),
        P(None, DP, TP),
        P(None, TP),
        P(None, DP, TP),
        P(None, DP, TP),
        P(None, DP, TP),
        P(None, TP, DP),
        P(None, DP, None, TP),
    )
    out_specs = (P(TP, DP), P(None, DP, None, TP))
    return jax.shard_map(shards, mesh=fine, in_specs=in_specs, out_specs=out_specs, check_vma=False)
```

```python
import functools

import jax
import jax.numpy as jnp
from jax import lax
from jax.experimental import pallas as pl
from jax.experimental.pallas import tpu as pltpu
from jax.sharding import Mesh, PartitionSpec as P

D = 4096
DK = 128
BLOCKS = 2
PAD = 8
LANES = 128
BF = jnp.bfloat16
F32 = jnp.float32
DP = ("y", "x")
TP = ("z", "c")
VMEM = pl.BlockSpec(memory_space=pltpu.VMEM)
SMALL = pltpu.CompilerParams(vmem_limit_bytes=12 * 1024 * 1024)


ORDER = {
    "z": tuple((8 + k) % 16 for k in range(16)),
    DP: tuple((10 + k) % 16 for k in range(16)),
}
ORDER[TP] = tuple(2 * z + c for z in ORDER["z"] for c in (0, 1))
SEQ_OF_ROW = (0, 3, 1, 4, 2, 5)


def exchange(parts, axis):
    return lax.all_to_all(parts, axis, 0, 0, tiled=True, axis_index_groups=[list(ORDER[axis])])


def shift_between():
    return (ORDER[DP][0] - ORDER["z"][0]) % len(ORDER["z"])


def project_kernel(b, pieces_ref, gain_ref, *refs):
    *weights, out_ref = refs
    groups = pieces_ref.shape[0] // 2
    pieces = pieces_ref[...].astype(F32)
    first, second = pieces[:, 0, :], pieces[:, 1, :]
    at = 2 * LANES
    mixed = jnp.concatenate([first[:, at:], second[:, :LANES]], axis=1)
    rows = jnp.concatenate([first[:, :at], mixed, second[:, LANES:]], axis=0).astype(BF)
    i = lax.broadcasted_iota(jnp.int32, (groups * PAD, rows.shape[0]), 0)
    column = lax.broadcasted_iota(jnp.int32, (groups * PAD, rows.shape[0]), 1)
    piece = 2 * (((i >> 3) + shift_between()) & (groups - 1)) + (i & 1)
    chosen = jnp.where(column == ((i & 7) >> 1) * 2 * groups + piece, 1.0, 0.0).astype(BF)
    rows = jnp.dot(chosen, rows, preferred_element_type=F32)
    squares = jnp.sum(rows * rows, axis=1, keepdims=True)
    hidden = (rows * gain_ref[b : b + 1, :].astype(F32)).astype(BF)
    tiles = []
    for w in weights:
        part = jnp.dot(hidden, w[b], preferred_element_type=F32)
        tiles += [part[:, k : k + LANES] for k in range(0, part.shape[1], LANES)]
    last = tiles.pop()
    row = lax.broadcasted_iota(jnp.int32, last.shape, 0) & 7
    lane = lax.broadcasted_iota(jnp.int32, last.shape, 1)
    spread_squares = jnp.broadcast_to(squares, last.shape)
    moved = [pltpu.roll(spread_squares, k, 0) for k in (6, 4, 2)]
    extra = [pltpu.roll(last, k, 0) for k in (6, 4, 2)]
    extra.append(jnp.where(lane == 0, moved[0], jnp.where(lane == 1, moved[1], moved[2])))
    for k, tile in enumerate(tiles):
        if k < len(extra):
            tile = jnp.where(row >= 6, extra[k], tile)
        out_ref[:, :, k * LANES : (k + 1) * LANES] = tile.reshape(groups, PAD, LANES).astype(BF)


def project(b, pieces, gain, weights):
    cols = sum(w.shape[2] for w in weights) - LANES
    return pl.pallas_call(
        functools.partial(project_kernel, b),
        out_shape=jax.ShapeDtypeStruct((pieces.shape[0] // 2, PAD, cols), BF),
        in_specs=[VMEM] * (2 + len(weights)),
        out_specs=VMEM,
        compiler_params=SMALL,
        name="project",
    )(pieces, gain, *weights)


def spread_kernel(rows_ref, out_ref, own_ref):
    rows = rows_ref[...].astype(F32)
    first = jnp.concatenate([rows[0:1], rows[1:2, :LANES]], axis=1)
    second = jnp.concatenate([rows[1:2, LANES:], rows[2:3]], axis=1)
    own = jnp.concatenate([first, second], axis=0)
    own_ref[...] = own.astype(BF)
    out_ref[...] = jnp.broadcast_to(own[None], out_ref.shape).astype(BF)


def spread(rows, n):
    piece = (2, rows.size // 2)
    return pl.pallas_call(
        spread_kernel,
        out_shape=(jax.ShapeDtypeStruct((n, *piece), BF), jax.ShapeDtypeStruct(piece, BF)),
        in_specs=[VMEM],
        out_specs=(VMEM, VMEM),
        compiler_params=SMALL,
        name="spread",
    )(rows)


def hold_kernel(in_ref, out_ref):
    out_ref[0] = in_ref[0]


def hold(copies):
    return pl.pallas_call(
        hold_kernel,
        out_shape=jax.ShapeDtypeStruct(copies.shape, copies.dtype),
        in_specs=[VMEM],
        out_specs=VMEM,
        input_output_aliases={0: 0},
        compiler_params=SMALL,
        cost_estimate=pl.CostEstimate(flops=10**10, bytes_accessed=10**7, transcendentals=0),
        name="hold",
    )(copies)


def finish_kernel(heads_ref, stream_ref, out_ref):
    total = jnp.sum(heads_ref[...].astype(F32), axis=0) + stream_ref[...].astype(F32)
    first, second = total[0:1], total[1:2]
    at = 2 * LANES
    middle = jnp.concatenate([first[:, at:], second[:, :LANES]], axis=1)
    out_ref[...] = jnp.concatenate([first[:, :at], middle, second[:, LANES:]], axis=0).astype(BF)


def finish(heads, stream, shape):
    return pl.pallas_call(
        finish_kernel,
        out_shape=jax.ShapeDtypeStruct(shape, BF),
        in_specs=[VMEM] * 2,
        out_specs=VMEM,
        compiler_params=SMALL,
        name="finish",
    )(heads, stream)


def step_kernel(b, seqs, kc, vc, parts_ref, shift_ref, fade_ref, state_ref, out_ref, d_ref, k_ref, v_ref):
    total = jnp.sum(parts_ref[...].astype(F32), axis=0)
    tiles = [total[:, k : k + LANES] for k in range(0, total.shape[1], LANES)]
    row = lax.broadcasted_iota(jnp.int32, tiles[0].shape, 0)
    lane = lax.broadcasted_iota(jnp.int32, tiles[0].shape, 1)

    def from_blank(first, second, third):
        second, third = pltpu.roll(second, 4, 0), pltpu.roll(third, 6, 0)
        return jnp.where(row < 2, pltpu.roll(first, 2, 0), jnp.where(row < 4, second, third))

    tiles.append(from_blank(*tiles[:3]))
    squares = jnp.where(lane == row >> 1, from_blank(*tiles[3:4] * 3), 0.0)
    inv_rms = lax.rsqrt(jnp.sum(squares, axis=1, keepdims=True)[:seqs] / D + 1e-06)
    total = jnp.concatenate(tiles, axis=1)[:seqs] * inv_rms
    cols = 3 * kc + 2 * vc
    queries = total[:, :kc] * DK ** (-0.5)
    keys = total[:, kc : 2 * kc]
    pre = total[:, 2 * kc : 3 * kc] + shift_ref[b : b + 1, :]
    values = total[:, 3 * kc : 3 * kc + vc]
    gates = total[:, 3 * kc + vc : cols]
    log_sigmoid = jnp.minimum(pre, 0.0) - jnp.log1p(jnp.exp(-jnp.abs(pre)))
    fade = jnp.concatenate([fade_ref[s : s + 1, b, :] for s in SEQ_OF_ROW], axis=0)
    decay = jnp.exp(log_sigmoid / 16.0 + fade)
    fresh_part = jnp.sum(queries * keys, axis=1, keepdims=True) * values
    columns = jnp.concatenate([queries * decay, jnp.zeros((PAD - seqs, kc), F32)], axis=0).T
    old = [
        jnp.sum(columns[:, j : j + 1] * state_ref[b, s], axis=0, keepdims=True)
        for j, s in enumerate(SEQ_OF_ROW)
    ]
    readout = jnp.concatenate(old, axis=0) + fresh_part
    gated = readout * (gates / (1.0 + jnp.exp(-gates)))
    chunks = [gated[j : j + 1, k : k + LANES] for j in range(seqs) for k in range(0, vc, LANES)]
    packed = [jnp.concatenate(chunks[k : k + 3], axis=1) for k in range(0, len(chunks), 3)]
    out_ref[...] = jnp.broadcast_to(jnp.concatenate(packed, axis=0)[None], out_ref.shape).astype(BF)
    for j, s in enumerate(SEQ_OF_ROW):
        d_ref[s : s + 1] = decay[j : j + 1]
        k_ref[s : s + 1] = keys[j : j + 1]
        v_ref[s : s + 1] = values[j : j + 1]


def step(b, parts, shift, fade, state):
    seqs, _, kc = fade.shape
    vc = state.shape[3]
    return pl.pallas_call(
        functools.partial(step_kernel, b, seqs, kc, vc),
        out_shape=(
            jax.ShapeDtypeStruct((parts.shape[0], seqs * vc // (3 * LANES), 3 * LANES), BF),
            jax.ShapeDtypeStruct((seqs, kc), F32),
            jax.ShapeDtypeStruct((seqs, kc), F32),
            jax.ShapeDtypeStruct((seqs, vc), F32),
        ),
        in_specs=[VMEM] * 4,
        out_specs=(VMEM,) * 4,
        compiler_params=SMALL,
        name="step",
    )(parts, shift, fade, state)


def readback_kernel(b, gated_ref, weight_ref, out_ref):
    groups, packed, width = gated_ref.shape
    flat = gated_ref[...].astype(F32).reshape(groups * packed, width).astype(BF)
    chunks = jnp.concatenate([flat[:, k : k + LANES] for k in range(0, width, LANES)], axis=0)
    i = lax.broadcasted_iota(jnp.int32, (6 * groups, chunks.shape[0]), 0)
    column = lax.broadcasted_iota(jnp.int32, (6 * groups, chunks.shape[0]), 1)
    piece = lax.rem(i, 2 * groups)
    group = ((piece >> 1) + groups - shift_between()) & (groups - 1)
    halves = []
    for half in (0, 1):
        chunk = 4 * lax.div(i, 2 * groups) + 2 * (piece & 1) + half
        row = (chunk * 11) >> 5
        source = ((chunk - 3 * row) * groups + group) * packed + row
        chosen = jnp.where(column == source, 1.0, 0.0).astype(BF)
        halves.append(jnp.dot(chosen, chunks, preferred_element_type=F32))
    gated = jnp.concatenate(halves, axis=1).astype(BF)
    branch = jnp.dot(gated, weight_ref[b], preferred_element_type=F32)
    one, two, three = (branch[k * 2 * groups : (k + 1) * 2 * groups] for k in range(3))
    first = jnp.concatenate([one, two[:, :LANES]], axis=1)
    second = jnp.concatenate([two[:, LANES:], three], axis=1)
    out_ref[...] = jnp.stack([first, second], axis=1).astype(BF)


def readback(b, gated, weight):
    groups = gated.shape[0]
    return pl.pallas_call(
        functools.partial(readback_kernel, b),
        out_shape=jax.ShapeDtypeStruct((2 * groups, 2, 3 * weight.shape[2] // 2), BF),
        in_specs=[VMEM] * 2,
        out_specs=VMEM,
        compiler_params=SMALL,
        name="readback",
    )(gated, weight)


def shards(
    incoming_embeddings,
    rescale_factors,
    probe_lift,
    address_lift,
    forget_lift,
    forget_shift,
    surplus_fade,
    content_lift,
    filter_lift,
    readback_lift,
    memory_tensor,
):
    weights = (probe_lift, address_lift, forget_lift, content_lift, filter_lift)
    depth = lax.axis_size("z")
    fade = jnp.transpose(surplus_fade, (1, 0, 2))
    copies, stream = spread(incoming_embeddings, 2 * depth)
    copies = hold(copies)
    kept = []
    for b in range(BLOCKS):
        pieces = exchange(copies, TP)
        parts = exchange(project(b, pieces, rescale_factors, weights), DP)
        gated, *small = step(b, parts, forget_shift, fade, memory_tensor)
        kept.append(small)
        gathered = exchange(gated, DP)
        if b == BLOCKS - 1:
            gathered, kept = lax.optimization_barrier((gathered, kept))
        heads = exchange(readback(b, gathered, readback_lift), TP)
        if b == BLOCKS - 1:
            mixed = finish(heads, stream, incoming_embeddings.shape)
            break
        branch = jnp.sum(heads.astype(F32), axis=0)
        stream = (stream.astype(F32) + branch).astype(BF)
        copies = jnp.broadcast_to(stream[None], copies.shape)
    fresh = [
        memory_tensor[b] * d[:, :, None] + k[:, :, None] * v[:, None, :]
        for b, (d, k, v) in enumerate(kept)
    ]
    return mixed, jnp.stack(fresh)


def solution(mesh):
    z = mesh.shape["tp"] // 2
    fine = Mesh(mesh.devices.reshape(z, 2, 4, 4), ("z", "c", "y", "x"))
    in_specs = (
        P(TP, DP),
        P(None, DP),
        P(None, DP, TP),
        P(None, DP, TP),
        P(None, DP, TP),
        P(None, TP),
        P(None, DP, TP),
        P(None, DP, TP),
        P(None, DP, TP),
        P(None, TP, DP),
        P(None, DP, None, TP),
    )
    out_specs = (P(TP, DP), P(None, DP, None, TP))
    return jax.shard_map(shards, mesh=fine, in_specs=in_specs, out_specs=out_specs, check_vma=False)
```
